128 devices in a mesh: ep: 128 (over z, y, x, core).
Axes of the slice: x: 4, y: 4, z: 4, core: 2. Of those that a mesh axis runs over, the one named last changes fastest.
Arguments:
- tokens: bfloat16 [2048, 1024], P('ep'), may hold values from -6 to 6
- lengths: int32 [2048], P('ep'), may hold values from 1 to 8191
- cache_keys: bfloat16 [2048, 128, 512], P('ep'), may hold values from -6 to 6
- cache_values: bfloat16 [2048, 128, 1024], P('ep'), may hold values from -6 to 6
- retention_state: float32 [2048, 4, 128, 256], P('ep'), may hold values from -24 to 24
- mix_gain: float32 [1024], replicated, may hold values from 0.1 to 1.9
- query_weight: bfloat16 [1024, 512], replicated, may hold values from -0.1875 to 0.1875
- key_weight: bfloat16 [1024, 512], replicated, may hold values from -0.1875 to 0.1875
- value_weight: bfloat16 [1024, 1024], replicated, may hold values from -0.1875 to 0.1875
- out_weight: bfloat16 [1024, 1024], replicated, may hold values from -0.1875 to 0.1875
- ffn_gain: float32 [1024], replicated, may hold values from 0.1 to 1.9
- routes: int32 [2048, 6], P('ep'), may hold values from 0 to 127, all different within a row; in each aligned block of 16 rows (0 to 15, 16 to 31, ...) at most 2 rows name the same one
- route_scores: float32 [2048, 6], P('ep'), may hold values from 0.05 to 1
- expert_gate: bfloat16 [128, 1024, 256], P('ep'), may hold values from -0.1875 to 0.1875
- expert_up: bfloat16 [128, 1024, 256], P('ep'), may hold values from -0.1875 to 0.1875
- expert_down: bfloat16 [128, 256, 1024], P('ep'), may hold values from -0.375 to 0.375
- shared_gate: bfloat16 [1024, 256], replicated, may hold values from -0.1875 to 0.1875
- shared_up: bfloat16 [1024, 256], replicated, may hold values from -0.1875 to 0.1875
- shared_down: bfloat16 [256, 1024], replicated, may hold values from -0.375 to 0.375
- dense_gate: bfloat16 [4096, 1024], P('ep'), may hold values from -0.1875 to 0.1875
- dense_up: bfloat16 [4096, 1024], P('ep'), may hold values from -0.1875 to 0.1875
- dense_down: bfloat16 [4096, 1024], P('ep'), may hold values from -0.09375 to 0.09375
- dense_mix: float32 [1024], replicated, may hold values from -3 to 3
Outputs:
- layer_out: bfloat16 [2048, 1024], P('ep')
- new_keys: bfloat16 [2048, 512], P('ep')
- new_values: bfloat16 [2048, 1024], P('ep')
The draws below stay inside these ranges and needn't reach their ends.
Inputs may be any that keep to these rules, and one draw needn't show every extreme that they name: `routes`: each row names 6 different experts; among the rows of one device no expert is named more than 2 times.
All inputs are finite; a program needn't handle non-finite values.
Results may differ from the reference program's by a relative error of at most 0.012.
Values may be sent and summed in bfloat16 or wider, within the bound.
No kernel may reach another device: no remote copies, remote signals or barrier semaphores. Data moves between devices by JAX's collectives and lax.ppermute only.
A program may use at most 128 MiB of HBM per device.

```python
import math
import jax
import jax.numpy as jnp
import numpy as np
from jax import lax

D = 1024
HEADS = 4
DK = 128
DV = 256
BLOCK = 128
SEQ_DEV = 16
SEQS = 2048
EXPERTS = 128
TOP_K = 6
CAP = 2
EH = 256
SH = 256
DENSE_FF = 4096
N_EP = 128


def plant(values, stream_key, smallest, top_value):
    dims = values.shape
    spot = [jax.random.randint(jax.random.fold_in(stream_key, axis), (), 0, dims[axis]) for axis in range(len(dims))]
    values = values.at[tuple(spot)].set(smallest)
    longest = dims.index(max(dims))
    spot[longest] = (spot[longest] + 1) % dims[longest]
    return values.at[tuple(spot)].set(top_value)


def shard_levels(rng, dims, shards, low, high):
    factor_of = 1.0
    for axis_at, shards_of in shards:
        heights = jax.random.uniform(jax.random.fold_in(jax.random.fold_in(rng, 6), axis_at), (shards_of,), jnp.float32, low / len(shards), high / len(shards))
        factor_of = factor_of * jnp.repeat(jnp.exp(heights), dims[axis_at] // shards_of).reshape((-1,) + (1,) * (len(dims) - 1 - axis_at))
    return factor_of


def routed_block(key, own, number, rows, count, top, reach, slope):
    sequence = jax.random.permutation(key, count)
    crowded, common = portions_of(count, rows * top, reach, slope, True), portions_of(count, rows * top, reach, slope, False)
    places = jnp.arange(count)

    def named(tallies, offset_by):
        used = int((tallies > 0).sum())
        fixed = max(1, used // 4)
        passed = fixed + (places - fixed + offset_by * (used - fixed)) % max(1, count - fixed)
        return jnp.zeros((count,), jnp.int32).at[sequence[jnp.where(places < fixed, places, passed)]].set(jnp.asarray(tallies, jnp.int32))

    tallies = jnp.where(number % 4 == 0, named(crowded, number // 4), named(common, number - number // 4 - 1))
    mixed = jax.random.permutation(jax.random.fold_in(own, 3), count)
    donor, receiver = mixed[0:count // 2 * 2:2], mixed[1:count // 2 * 2:2]
    room = jnp.minimum(tallies[donor] - 1, reach - tallies[receiver]) // 2
    room = jnp.where((donor == sequence[0]) | (receiver == sequence[0]) | (tallies[receiver] == 0), 0, jnp.maximum(room, 0))
    passed = jax.random.randint(jax.random.fold_in(own, 4), (count // 2,), 0, 1 << 20) % (room + 1)
    tallies = tallies.at[donor].add(-passed).at[receiver].add(passed)
    members = jnp.searchsorted(jnp.cumsum(tallies), jnp.arange(rows * top), side="right").astype(jnp.int32)
    grid = members.reshape(top, rows).T
    grid = grid[jax.random.permutation(jax.random.fold_in(own, 1), rows)]
    offset_by = jax.random.randint(jax.random.fold_in(own, 2), (rows, 1), 0, top)
    return jnp.take_along_axis(grid, (jnp.arange(top)[None, :] + offset_by) % top, axis=1)


def portions_of(amount, total, limit, slope, full):
    portions = [(1 << 20) // math.isqrt(grade ** slope) + 1 for grade in range(1, amount + 1)]
    largest = limit if full else min(limit, max(-(-total // amount), total * portions[0] // sum(portions)))
    least = 1 if total - largest >= amount - 1 else 0
    counts, surplus = [largest] + [least] * (amount - 1), total - largest - least * (amount - 1)
    while surplus > 0:
        free = [i for i in range(1, amount) if counts[i] < largest] or [i for i in range(1, amount) if counts[i] < limit]
        pool, budget = sum([portions[i] for i in free]), surplus
        for i in free:
            addition = min(limit - counts[i], max(1, budget * portions[i] // pool), surplus)
            counts[i] = counts[i] + addition
            surplus = surplus - addition
    return np.array(counts)


def gaussian(own_key, dims, deviation, reach, shards=(), held_as=jnp.bfloat16):
    result = deviation * jax.random.normal(own_key, dims, jnp.float32)
    if shards:
        result = result * shard_levels(own_key, dims, shards, -0.22, 0.18)
    return jnp.clip(result, -reach, reach).astype(held_as)


def setup_inputs(seed: int = 0) -> dict:
    key_of = jax.random.split(jax.random.key(seed), 24)
    tokens = gaussian(key_of[0], (SEQS, D), 1.0, 6.0, ((0, 128),))
    lengths = plant(jax.random.randint(key_of[1], (SEQS,), 1, 8192), jax.random.fold_in(key_of[1], 1), 1, 8191).astype(jnp.int32)
    cache_keys = gaussian(key_of[2], (SEQS, BLOCK, HEADS * DK), 1.0, 6.0, ((0, 128),))
    cache_values = gaussian(key_of[3], (SEQS, BLOCK, HEADS * DV), 1.0, 6.0, ((0, 128),))
    retention_state = gaussian(key_of[4], (SEQS, HEADS, DK, DV), 4.0, 24.0, ((0, 128),), jnp.float32)
    mix_gain = jnp.clip(1.0 + 0.18 * jax.random.normal(key_of[5], (D,), jnp.float32), 0.1, 1.9)
    query_weight = gaussian(key_of[6], (D, HEADS * DK), D ** -0.5, 0.1875)
    key_weight = gaussian(key_of[7], (D, HEADS * DK), D ** -0.5, 0.1875)
    value_weight = gaussian(key_of[8], (D, HEADS * DV), D ** -0.5, 0.1875)
    out_weight = gaussian(key_of[9], (HEADS * DV, D), (HEADS * DV) ** -0.5, 0.1875)
    ffn_gain = jnp.clip(1.0 + 0.18 * jax.random.normal(key_of[10], (D,), jnp.float32), 0.1, 1.9)
    routes_keys = jax.random.split(jax.random.fold_in(key_of[11], 1), SEQS // SEQ_DEV)
    routes_turns = jax.random.permutation(jax.random.fold_in(key_of[11], 3), SEQS // SEQ_DEV)
    routes = jax.vmap(lambda own, number: routed_block(jax.random.fold_in(key_of[11], 2), own, number, SEQ_DEV, EXPERTS, TOP_K, CAP, 1))(routes_keys, routes_turns).reshape((SEQS, TOP_K))
    route_scores = jnp.clip(0.05 + 0.95 * jax.random.uniform(key_of[12], (SEQS, TOP_K), jnp.float32) ** shard_levels(key_of[12], (SEQS, TOP_K), ((0, 128),), -0.2, 0.2), 0.05, 1.0)
    expert_gate = gaussian(key_of[13], (EXPERTS, D, EH), D ** -0.5, 0.1875, ((0, 128),))
    expert_up = gaussian(key_of[14], (EXPERTS, D, EH), D ** -0.5, 0.1875, ((0, 128),))
    expert_down = gaussian(key_of[15], (EXPERTS, EH, D), EH ** -0.5, 0.375, ((0, 128),))
    shared_gate = gaussian(key_of[16], (D, SH), D ** -0.5, 0.1875)
    shared_up = gaussian(key_of[17], (D, SH), D ** -0.5, 0.1875)
    shared_down = gaussian(key_of[18], (SH, D), SH ** -0.5, 0.375)
    dense_gate = gaussian(key_of[19], (DENSE_FF, D), D ** -0.5, 0.1875, ((0, 128),))
    dense_up = gaussian(key_of[20], (DENSE_FF, D), D ** -0.5, 0.1875, ((0, 128),))
    dense_down = gaussian(key_of[21], (DENSE_FF, D), DENSE_FF ** -0.5, 0.09375, ((0, 128),))
    dense_mix = jnp.clip(jax.random.uniform(key_of[22], (D,), jnp.float32, -3.0, 3.0), -3.0, 3.0)
    return {"tokens": tokens, "lengths": lengths, "cache_keys": cache_keys, "cache_values": cache_values, "retention_state": retention_state, "mix_gain": mix_gain, "query_weight": query_weight, "key_weight": key_weight, "value_weight": value_weight, "out_weight": out_weight, "ffn_gain": ffn_gain, "routes": routes, "route_scores": route_scores, "expert_gate": expert_gate, "expert_up": expert_up, "expert_down": expert_down, "shared_gate": shared_gate, "shared_up": shared_up, "shared_down": shared_down, "dense_gate": dense_gate, "dense_up": dense_up, "dense_down": dense_down, "dense_mix": dense_mix}


eps = 1e-06
route_scale = 2.5
rope_base = 10000.0

def normed(values):
    return values * lax.rsqrt(lax.optimization_barrier(jnp.mean(values * values, axis=-1, keepdims=True)) + eps)

def log_decay(head_count):
    return jnp.log1p(-jnp.exp2(-5.0 - jnp.arange(head_count, dtype=jnp.float32)))

def rotate(values, positions):
    half_size = values.shape[-1] // 2
    inverse = rope_base ** (-jnp.arange(half_size, dtype=jnp.float32) / half_size)
    angles = positions.astype(jnp.float32)[:, None, None] * inverse[None, None, :]
    cosine = jnp.cos(angles)
    sine_part = jnp.sin(angles)
    first_half = values[..., :half_size]
    second = values[..., half_size:]
    return jnp.concatenate([first_half * cosine - second * sine_part, first_half * sine_part + second * cosine], axis=-1)

def swiglu(inputs, w_gate, w_up, w_down):
    gate_part = jnp.dot(inputs, w_gate, preferred_element_type=jnp.float32)
    up_part = jnp.dot(inputs, w_up, preferred_element_type=jnp.float32)
    hidden = (jax.nn.silu(gate_part) * up_part).astype(jnp.bfloat16)
    return jnp.dot(hidden, w_down, preferred_element_type=jnp.float32)

def retain(tokens, lengths, mix_gain, w_query, w_key, w_value, w_out, cache_keys, cache_values, carry_state):
    seq_count, head_count, key_size, value_size = carry_state.shape
    block_size = cache_keys.shape[1]
    widened = tokens.astype(jnp.float32)
    normal_in = (normed(widened) * mix_gain).astype(jnp.bfloat16)
    raw_query = jnp.dot(normal_in, w_query, preferred_element_type=jnp.float32).reshape(seq_count, head_count, key_size)
    raw_key = jnp.dot(normal_in, w_key, preferred_element_type=jnp.float32).reshape(seq_count, head_count, key_size)
    raw_value = jnp.dot(normal_in, w_value, preferred_element_type=jnp.float32).reshape(seq_count, head_count, value_size)
    queries = (rotate(raw_query, lengths) * key_size ** (-0.5)).astype(jnp.bfloat16)
    new_keys = rotate(raw_key, lengths).astype(jnp.bfloat16)
    new_values = raw_value.astype(jnp.bfloat16)
    filled = lengths % block_size
    decay_rate = log_decay(head_count)
    places = jnp.arange(block_size, dtype=jnp.int32)
    stored_keys = cache_keys.reshape(seq_count, block_size, head_count, key_size)
    stored_values = cache_values.reshape(seq_count, block_size, head_count, value_size)
    scores = jnp.einsum('shd,sjhd->shj', queries.astype(jnp.float32), stored_keys.astype(jnp.float32))
    distance = jnp.maximum(filled[:, None] - places[None, :], 0).astype(jnp.float32)
    live_mask = places[None, :] < filled[:, None]
    weighted = jnp.where(live_mask[:, None, :], scores * jnp.exp(distance[:, None, :] * decay_rate[None, :, None]), 0.0).astype(jnp.bfloat16)
    own_weight = lax.optimization_barrier(jnp.sum(queries.astype(jnp.float32) * new_keys.astype(jnp.float32), axis=-1)).astype(jnp.bfloat16)
    inside = jnp.einsum('shj,sjhe->she', weighted.astype(jnp.float32), stored_values.astype(jnp.float32))
    inside = inside + own_weight.astype(jnp.float32)[:, :, None] * new_values.astype(jnp.float32)
    carried = jnp.einsum('shd,shde->she', queries.astype(jnp.float32), carry_state, precision=lax.Precision.HIGHEST)
    carried = carried * jnp.exp((filled.astype(jnp.float32)[:, None] + 1.0) * decay_rate[None, :])[:, :, None]
    headed = normed(inside + carried).astype(jnp.bfloat16).reshape(seq_count, head_count * value_size)
    mixer_out = jnp.dot(headed, w_out, preferred_element_type=jnp.float32)
    residual = widened + normed(mixer_out)
    return (residual, new_keys.reshape(seq_count, head_count * key_size), new_values.reshape(seq_count, head_count * value_size))

def reference(tokens, lengths, cache_keys, cache_values, retention_state, mix_gain, query_weight, key_weight, value_weight, out_weight, ffn_gain, routes, route_scores, expert_gate, expert_up, expert_down, shared_gate, shared_up, shared_down, dense_gate, dense_up, dense_down, dense_mix):
    residual, new_keys, new_values = retain(tokens, lengths, mix_gain, query_weight, key_weight, value_weight, out_weight, cache_keys, cache_values, retention_state)
    normal_ffn = (normed(residual) * ffn_gain).astype(jnp.bfloat16)
    shared_out = swiglu(normal_ffn, shared_gate, shared_up, shared_down)
    dense_gate_part = jnp.dot(normal_ffn, dense_gate.T, preferred_element_type=jnp.float32)
    dense_up_part = jnp.dot(normal_ffn, dense_up.T, preferred_element_type=jnp.float32)
    dense_hidden = (jax.nn.silu(dense_gate_part) * dense_up_part).astype(jnp.bfloat16)
    dense_out = jnp.dot(dense_hidden, dense_down, preferred_element_type=jnp.float32)
    route_weight = route_scores / lax.optimization_barrier(jnp.sum(route_scores, axis=-1, keepdims=True)) * route_scale
    flat_routes = routes.reshape(-1)
    flat_weight = route_weight.reshape(-1)
    most_rows = N_EP * CAP
    slot_rank = jnp.arange(most_rows, dtype=jnp.int32)

    def one_expert(running, expert_id):
        hits = flat_routes == expert_id
        hit_count = jnp.sum(hits.astype(jnp.int32))
        picked = jnp.nonzero(hits, size=most_rows, fill_value=0)[0].astype(jnp.int32)
        is_valid = slot_rank < hit_count
        row_ids = picked // TOP_K
        outputs = swiglu(normal_ffn[row_ids], expert_gate[expert_id], expert_up[expert_id], expert_down[expert_id]).astype(jnp.bfloat16)
        added = jnp.where(is_valid[:, None], outputs.astype(jnp.float32) * flat_weight[picked][:, None], 0.0)
        return (running.at[row_ids].add(added), None)
    routed, _ = lax.scan(one_expert, jnp.zeros(residual.shape, jnp.float32), jnp.arange(EXPERTS, dtype=jnp.int32))
    combined = shared_out + routed + jax.nn.sigmoid(dense_mix) * dense_out
    layer_out = (residual + normed(combined)).astype(jnp.bfloat16)
    return (layer_out, new_keys, new_values)
```

```python
import jax
import jax.numpy as jnp
from jax import lax
from jax.sharding import PartitionSpec as P


eps = 1e-06
route_scale = 2.5
rope_base = 10000.0


def flip(values, mask):
    return lax.ppermute(values, "ep", [(i, i ^ mask) for i in range(lax.axis_size("ep"))])


def spread(values, masks):
    return jnp.concatenate([values] + [flip(values, m) for m in masks], axis=0)


def fold(values, masks):
    pieces = values.reshape((len(masks) + 1, -1) + values.shape[1:])
    total = pieces[0].astype(jnp.float32)
    for k, m in enumerate(masks):
        total = total + flip(pieces[k + 1], m).astype(jnp.float32)
    return total.astype(jnp.bfloat16)


x_masks = (2, 4, 6)
y_masks = (8, 16, 24)
z_masks = (32, 64, 96)


def normed(values):
    return values * lax.rsqrt(jnp.mean(values * values, axis=-1, keepdims=True) + eps)


def log_decay(head_count):
    return jnp.log1p(-jnp.exp2(-5.0 - jnp.arange(head_count, dtype=jnp.float32)))


def rotate(values, positions):
    half_size = values.shape[-1] // 2
    inverse = rope_base ** (-jnp.arange(half_size, dtype=jnp.float32) / half_size)
    angles = positions.astype(jnp.float32)[:, None, None] * inverse[None, None, :]
    cosine = jnp.cos(angles)
    sine_part = jnp.sin(angles)
    first_half = values[..., :half_size]
    second = values[..., half_size:]
    return jnp.concatenate(
        [first_half * cosine - second * sine_part, first_half * sine_part + second * cosine],
        axis=-1,
    )


def swiglu(inputs, w_gate, w_up, w_down):
    gate_part = jnp.dot(inputs, w_gate, preferred_element_type=jnp.float32)
    up_part = jnp.dot(inputs, w_up, preferred_element_type=jnp.float32)
    hidden = (jax.nn.silu(gate_part) * up_part).astype(jnp.bfloat16)
    return jnp.dot(hidden, w_down, preferred_element_type=jnp.float32)


def dense_part(inputs, gate_rows, up_rows, down_rows):
    contract = (((1,), (1,)), ((), ()))
    gate_part = lax.dot_general(inputs, gate_rows, contract, preferred_element_type=jnp.float32)
    up_part = lax.dot_general(inputs, up_rows, contract, preferred_element_type=jnp.float32)
    hidden = (jax.nn.silu(gate_part) * up_part).astype(jnp.bfloat16)
    return jnp.dot(hidden, down_rows, preferred_element_type=jnp.float32)


def retain(
    tokens, lengths, mix_gain, w_query, w_key, w_value, w_out, cache_keys, cache_values, carry_state
):
    seq_count, head_count, key_size, value_size = carry_state.shape
    block_size = cache_keys.shape[1]
    widened = tokens.astype(jnp.float32)
    normal_in = (normed(widened) * mix_gain).astype(jnp.bfloat16)
    raw_query = jnp.dot(normal_in, w_query, preferred_element_type=jnp.float32).reshape(
        seq_count, head_count, key_size
    )
    raw_key = jnp.dot(normal_in, w_key, preferred_element_type=jnp.float32).reshape(
        seq_count, head_count, key_size
    )
    raw_value = jnp.dot(normal_in, w_value, preferred_element_type=jnp.float32).reshape(
        seq_count, head_count, value_size
    )
    queries = (rotate(raw_query, lengths) * key_size ** (-0.5)).astype(jnp.bfloat16)
    new_keys = rotate(raw_key, lengths).astype(jnp.bfloat16)
    new_values = raw_value.astype(jnp.bfloat16)
    filled = lengths % block_size
    decay_rate = log_decay(head_count)
    places = jnp.arange(block_size, dtype=jnp.int32)
    stored_keys = cache_keys.reshape(seq_count, block_size, head_count, key_size)
    stored_values = cache_values.reshape(seq_count, block_size, head_count, value_size)
    scores = jnp.einsum("shd,sjhd->shj", queries, stored_keys, preferred_element_type=jnp.float32)
    distance = jnp.maximum(filled[:, None] - places[None, :], 0).astype(jnp.float32)
    live_mask = places[None, :] < filled[:, None]
    weighted = jnp.where(
        live_mask[:, None, :],
        scores * jnp.exp(distance[:, None, :] * decay_rate[None, :, None]),
        0.0,
    ).astype(jnp.bfloat16)
    own_weight = jnp.sum(
        queries.astype(jnp.float32) * new_keys.astype(jnp.float32), axis=-1
    ).astype(jnp.bfloat16)
    inside = jnp.einsum(
        "shj,sjhe->she", weighted, stored_values, preferred_element_type=jnp.float32
    )
    inside = inside + own_weight.astype(jnp.float32)[:, :, None] * new_values.astype(jnp.float32)
    carried = jnp.einsum("shd,shde->she", queries.astype(jnp.float32), carry_state)
    carried = (
        carried
        * jnp.exp((filled.astype(jnp.float32)[:, None] + 1.0) * decay_rate[None, :])[:, :, None]
    )
    headed = (
        normed(inside + carried).astype(jnp.bfloat16).reshape(seq_count, head_count * value_size)
    )
    mixer_out = jnp.dot(headed, w_out, preferred_element_type=jnp.float32)
    residual = widened + normed(mixer_out)
    return (
        residual,
        new_keys.reshape(seq_count, head_count * key_size),
        new_values.reshape(seq_count, head_count * value_size),
    )


def capacity(seq_count, top_count, expert_count):
    return max(2, seq_count * top_count * 8 // (3 * expert_count))


def exchanged_experts(normal_ffn, routes, route_weight, expert_gate, expert_up, expert_down):
    seq_count, top_count = routes.shape
    model_width = normal_ffn.shape[1]
    expert_count = lax.axis_size("ep") * expert_gate.shape[0]
    slot_count = capacity(seq_count, top_count, expert_count)
    flat_routes = routes.reshape(-1)
    onehot = (flat_routes[:, None] == jnp.arange(expert_count, dtype=jnp.int32)[None, :]).astype(
        jnp.int32
    )
    slot_ids = jnp.sum((jnp.cumsum(onehot, axis=0) - 1) * onehot, axis=1)
    target = flat_routes * slot_count + slot_ids
    placed = (
        target[None, :] == jnp.arange(expert_count * slot_count, dtype=jnp.int32)[:, None]
    ).astype(jnp.float32)
    chosen = jnp.sum(placed.reshape(expert_count * slot_count, seq_count, top_count), axis=2)
    outgoing = jnp.dot(
        chosen.astype(jnp.bfloat16), normal_ffn, preferred_element_type=jnp.float32
    ).astype(jnp.bfloat16)
    outgoing = outgoing.reshape(expert_count, slot_count, model_width)
    arrived = lax.all_to_all(outgoing, "ep", split_axis=0, concat_axis=0, tiled=True)
    outputs = swiglu(
        arrived.reshape(-1, model_width), expert_gate[0], expert_up[0], expert_down[0]
    ).astype(jnp.bfloat16)
    returned = lax.all_to_all(
        outputs.reshape(arrived.shape), "ep", split_axis=0, concat_axis=0, tiled=True
    )
    weights_by_slot = placed * route_weight.reshape(-1)[None, :]
    combine = jnp.sum(
        weights_by_slot.reshape(expert_count * slot_count, seq_count, top_count), axis=2
    )
    return lax.dot_general(
        combine, returned.reshape(-1, model_width).astype(jnp.float32), (((0,), (0,)), ((), ()))
    )


def per_device(
    tokens,
    lengths,
    cache_keys,
    cache_values,
    retention_state,
    mix_gain,
    query_weight,
    key_weight,
    value_weight,
    out_weight,
    ffn_gain,
    routes,
    route_scores,
    expert_gate,
    expert_up,
    expert_down,
    shared_gate,
    shared_up,
    shared_down,
    dense_gate,
    dense_up,
    dense_down,
    dense_mix,
):
    residual, new_keys, new_values = retain(
        tokens,
        lengths,
        mix_gain,
        query_weight,
        key_weight,
        value_weight,
        out_weight,
        cache_keys,
        cache_values,
        retention_state,
    )
    normal_ffn = (normed(residual) * ffn_gain).astype(jnp.bfloat16)
    shared_out = swiglu(normal_ffn, shared_gate, shared_up, shared_down)
    gated = jax.nn.sigmoid(dense_mix)
    route_weight = route_scores / jnp.sum(route_scores, axis=-1, keepdims=True) * route_scale
    shard = jnp.stack([dense_gate, dense_up, dense_down])[None]
    weights = spread(spread(shard, x_masks), (1,))
    gate_rows, up_rows, down_rows = [
        weights[:, i].reshape(-1, dense_gate.shape[1]) for i in range(3)
    ]
    shared_tokens = spread(spread(normal_ffn, y_masks), z_masks)
    partial = gated * dense_part(shared_tokens, gate_rows, up_rows, down_rows)
    dense_out = fold(fold(partial.astype(jnp.bfloat16), z_masks), y_masks).astype(jnp.float32)
    combined = (
        shared_out
        + dense_out
        + exchanged_experts(normal_ffn, routes, route_weight, expert_gate, expert_up, expert_down)
    )
    layer_out = (residual + normed(combined)).astype(jnp.bfloat16)
    return (layer_out, new_keys, new_values)


def solution(mesh):
    in_specs = (
        P("ep", None),
        P("ep"),
        P("ep", None, None),
        P("ep", None, None),
        P("ep", None, None, None),
        P(),
        P(),
        P(),
        P(),
        P(),
        P(),
        P("ep", None),
        P("ep", None),
        P("ep", None, None),
        P("ep", None, None),
        P("ep", None, None),
        P(),
        P(),
        P(),
        P("ep", None),
        P("ep", None),
        P("ep", None),
        P(),
    )
    out_specs = (P("ep", None), P("ep", None), P("ep", None))
    return jax.shard_map(
        per_device, mesh=mesh, in_specs=in_specs, out_specs=out_specs, check_vma=False
    )
```

```python
import jax
import jax.numpy as jnp
from jax import lax
from jax.experimental import pallas as pl
from jax.experimental.pallas import tpu as pltpu
from jax.sharding import PartitionSpec as P


eps = 1e-06
route_scale = 2.5
rope_base = 10000.0

SEQ = 16
WIDTH = 1024
HEADS = 4
KEY = 128
VALUE = 256
BLOCK = 128
EXPERTS = 128
SLOTS = 2
CHUNKS = 8
PACKED = EXPERTS * CHUNKS * SLOTS
GROUP = 4

x_masks = (2, 4, 6)
y_masks = (8, 16, 24)
z_masks = (32, 64, 96)

f32 = jnp.float32
bf16 = jnp.bfloat16
vmem = pl.BlockSpec(memory_space=pltpu.VMEM)
hbm = pl.BlockSpec(memory_space=pl.ANY)
smem = pl.BlockSpec(memory_space=pltpu.SMEM)


def flip(values, mask):
    return lax.ppermute(values, "ep", [(i, i ^ mask) for i in range(lax.axis_size("ep"))])


def normed(values):
    return values * lax.rsqrt(jnp.mean(values * values, axis=-1, keepdims=True) + eps)


def dot(a, b):
    return jnp.dot(a, b, preferred_element_type=f32)


def dot_t(a, b):
    return lax.dot_general(a, b, (((1,), (1,)), ((), ())), preferred_element_type=f32)


def iota(shape, axis):
    return lax.broadcasted_iota(jnp.int32, shape, axis)


def silu(v):
    return v / (1.0 + jnp.exp(-v))


def head_rates(head_ids):
    return jnp.log1p(-jnp.exp2(-5.0 - head_ids.astype(f32)))


def rotary(lengths):
    half = KEY // 2
    inverse = rope_base ** (-jnp.arange(half, dtype=f32) / half)
    angles = lengths.astype(f32)[:, None] * inverse[None, :]
    cosine = jnp.cos(angles)
    sine = jnp.sin(angles)
    return jnp.concatenate([cosine, cosine], axis=1), jnp.concatenate([-sine, sine], axis=1)


def placement(routes, scores):
    expert = iota((SEQ, EXPERTS), 1)
    weight = scores / jnp.sum(scores, axis=1, keepdims=True) * route_scale
    named = jnp.zeros((SEQ, EXPERTS), f32)
    weighted = jnp.zeros((SEQ, EXPERTS), f32)
    for k in range(routes.shape[1]):
        hit = routes[:, k : k + 1] == expert
        named = jnp.where(hit, 1.0, named)
        weighted = jnp.where(hit, weight[:, k : k + 1], weighted)
    earlier = (iota((SEQ, SEQ), 1) < iota((SEQ, SEQ), 0)).astype(bf16)
    rank = dot(earlier, named.astype(bf16))
    first = jnp.where(rank < 0.5, named, 0.0)
    second = named - first
    column = iota((EXPERTS, PACKED), 1)
    row = iota((EXPERTS, PACKED), 0)
    same = row == column // (CHUNKS * SLOTS)
    even = column % SLOTS == 0
    to_first = (same & even).astype(bf16)
    to_second = (same & ~even).astype(bf16)

    def wide(factor):
        lanes = dot((first * factor).astype(bf16), to_first) + dot(
            (second * factor).astype(bf16), to_second
        )
        tall = jnp.broadcast_to(lanes[:, None, :], (SEQ, CHUNKS, PACKED)).reshape(
            SEQ * CHUNKS, PACKED
        )
        shape = (SEQ * CHUNKS, PACKED)
        match = iota(shape, 0) % CHUNKS == (iota(shape, 1) // SLOTS) % CHUNKS
        return jnp.where(match, tall, 0.0).astype(bf16)

    return wide(jnp.ones_like(weighted)), wide(weighted)


def mixer_kernel(
    filled_s,
    tokens,
    filled_v,
    cosine,
    sine,
    mix_gain,
    ffn_gain,
    routes,
    scores,
    keys_h,
    values_h,
    state_h,
    wq_h,
    wk_h,
    wv_h,
    wo_h,
    gate_h,
    up_h,
    down_h,
    residual_o,
    ffn_o,
    new_keys_o,
    new_values_o,
    outgoing_o,
    combine_o,
    shard_o,
    keys,
    values,
    state,
    wq,
    wk,
    wv,
    wo,
    weights_s,
    retained_s,
    chunk_s,
    sems,
    group_sems,
    shard_sems,
):
    def copy(src, dst, i):
        return pltpu.make_async_copy(src, dst, sems.at[i])

    qk_copies = [copy(wq_h, wq, 0), copy(wk_h, wk, 1)]
    key_copy = copy(keys_h, keys, 2)
    wv_copy = copy(wv_h, wv, 3)
    wo_copy = copy(wo_h, wo, 4)
    steps = SEQ // GROUP
    group_copies = []
    for g in range(steps):
        part = pl.ds(g * GROUP, GROUP)
        group_copies.append(
            (
                pltpu.make_async_copy(values_h.at[part], values.at[part], group_sems.at[0, g]),
                pltpu.make_async_copy(state_h.at[part], state.at[part], group_sems.at[1, g]),
            )
        )
    for c in qk_copies:
        c.start()
    key_copy.start()
    for c in group_copies[0]:
        c.start()
    wv_copy.start()
    for pair in group_copies[1:]:
        for c in pair:
            c.start()
    wo_copy.start()
    rows = gate_h.shape[0]
    shard_copies = [
        pltpu.make_async_copy(src, shard_o.at[pl.ds(i * rows, rows)], shard_sems.at[i])
        for i, src in enumerate((gate_h, up_h, down_h))
    ]
    for c in shard_copies:
        c.start()

    send, combine = placement(routes[...], scores[...])
    combine_o[...] = combine

    widened = tokens[...].astype(f32)
    normal_in = (normed(widened) * mix_gain[...]).astype(bf16)
    cos = jnp.concatenate([cosine[...]] * HEADS, axis=1)
    sin = jnp.concatenate([sine[...]] * HEADS, axis=1)

    def rotate(raw):
        swapped = jnp.concatenate(
            [pltpu.roll(raw[:, h * KEY : (h + 1) * KEY], KEY // 2, 1) for h in range(HEADS)],
            axis=1,
        )
        return raw * cos + swapped * sin

    for c in qk_copies:
        c.wait()
    queries = (rotate(dot(normal_in, wq[...])) * KEY ** (-0.5)).astype(bf16)
    new_keys = rotate(dot(normal_in, wk[...])).astype(bf16)
    new_keys_o[...] = new_keys
    queries32 = queries.astype(f32)
    product = queries32 * new_keys.astype(f32)

    head_of = iota((8, HEADS * KEY), 0)
    query_block = iota((8, HEADS * KEY), 1) // KEY == head_of
    place = iota((8, BLOCK), 1)
    rate_wide = head_rates(iota((8, BLOCK), 0))
    rate_tall = head_rates(iota((8, 1), 0))
    value_block = iota((8, HEADS * VALUE), 1) // VALUE == iota((8, HEADS * VALUE), 0)

    blocked = []
    key_copy.wait()
    for s in range(SEQ):
        spread_query = jnp.where(
            query_block, jnp.broadcast_to(queries32[s : s + 1], (8, HEADS * KEY)), 0.0
        ).astype(bf16)
        blocked.append(spread_query)
        found = dot_t(spread_query, keys[s])
        distance = jnp.maximum(filled_s[s] - place, 0).astype(f32)
        weights_s[s] = jnp.where(
            place < filled_s[s], found * jnp.exp(distance * rate_wide), 0.0
        ).astype(bf16)

    wv_waited = False
    for g in range(steps):
        for c in group_copies[g]:
            c.wait()
        for s in range(g * GROUP, (g + 1) * GROUP):
            inside = dot(weights_s[s], values[s])
            heads = blocked[s]
            stacked = (
                heads[:, 0:KEY]
                + heads[:, KEY : 2 * KEY]
                + heads[:, 2 * KEY : 3 * KEY]
                + heads[:, 3 * KEY : 4 * KEY]
            )
            carried = jnp.concatenate(
                [dot(stacked, state[s, h].astype(bf16)) for h in range(HEADS)], axis=1
            )
            decay = jnp.exp((filled_s[s].astype(f32) + 1.0) * rate_tall)
            both = jnp.where(value_block, inside + carried * decay, 0.0)
            retained_s[s : s + 1, :] = jnp.sum(both, axis=0, keepdims=True)

    wv_copy.wait()
    new_values = dot(normal_in, wv[...]).astype(bf16)
    new_values_o[...] = new_values
    new_values32 = new_values.astype(f32)
    headed = []
    for h in range(HEADS):
        own = jnp.sum(product[:, h * KEY : (h + 1) * KEY], axis=1, keepdims=True)
        own = own.astype(bf16).astype(f32)
        span = slice(h * VALUE, (h + 1) * VALUE)
        headed.append(normed(retained_s[:, span] + own * new_values32[:, span]).astype(bf16))
    wo_copy.wait()
    mixer_out = dot(jnp.concatenate(headed, axis=1), wo[...])
    residual = widened + normed(mixer_out)
    residual_o[...] = residual
    normal_ffn = (normed(residual) * ffn_gain[...]).astype(bf16)
    ffn_o[...] = normal_ffn
    chunk_s[...] = normal_ffn.astype(f32).reshape(SEQ * CHUNKS, WIDTH // CHUNKS)
    outgoing_o[...] = lax.dot_general(
        send, chunk_s[...].astype(bf16), (((0,), (0,)), ((), ())), preferred_element_type=f32
    ).astype(bf16)
    for c in shard_copies:
        c.wait()


def mixer(
    tokens,
    lengths,
    mix_gain,
    ffn_gain,
    routes,
    scores,
    cache_keys,
    cache_values,
    state,
    wq,
    wk,
    wv,
    wo,
    gate,
    up,
    down,
):
    filled = lengths % BLOCK
    cosine, sine = rotary(lengths)
    shapes = [
        jax.ShapeDtypeStruct((SEQ, WIDTH), f32),
        jax.ShapeDtypeStruct((SEQ, WIDTH), bf16),
        jax.ShapeDtypeStruct((SEQ, HEADS * KEY), bf16),
        jax.ShapeDtypeStruct((SEQ, WIDTH), bf16),
        jax.ShapeDtypeStruct((PACKED, WIDTH // CHUNKS), bf16),
        jax.ShapeDtypeStruct((SEQ * CHUNKS, PACKED), bf16),
        jax.ShapeDtypeStruct((3 * gate.shape[0], WIDTH), bf16),
    ]
    big = (cache_keys, cache_values, state, wq, wk, wv, wo)
    return pl.pallas_call(
        mixer_kernel,
        name="mixer",
        out_shape=shapes,
        in_specs=[smem] + [vmem] * 8 + [hbm] * 10,
        out_specs=[vmem] * 6 + [hbm],
        scratch_shapes=[pltpu.VMEM(a.shape, a.dtype) for a in big]
        + [
            pltpu.VMEM((SEQ, 8, BLOCK), bf16),
            pltpu.VMEM((SEQ, WIDTH), f32),
            pltpu.VMEM((SEQ * CHUNKS, WIDTH // CHUNKS), f32),
            pltpu.SemaphoreType.DMA((5,)),
            pltpu.SemaphoreType.DMA((2, SEQ // GROUP)),
            pltpu.SemaphoreType.DMA((3,)),
        ],
        cost_estimate=pl.CostEstimate(flops=2_000_000_000, bytes_accessed=22_000_000, transcendentals=0),
        compiler_params=pltpu.CompilerParams(vmem_limit_bytes=48 * 1024 * 1024),
    )(
        filled,
        tokens,
        filled[:, None],
        cosine,
        sine,
        mix_gain[None],
        ffn_gain[None],
        routes,
        scores,
        *big,
        gate,
        up,
        down,
    )


def swiglu(inputs, w_gate, w_up, w_down):
    hidden = (silu(dot(inputs, w_gate)) * dot(inputs, w_up)).astype(bf16)
    return dot(hidden, w_down)


def expert_kernel(arrived, gate, up, down, back, wide_s):
    wide_s[...] = arrived[...].astype(f32)
    period = CHUNKS * SLOTS
    rows = []
    for slot in range(SLOTS):
        rows.append(
            jnp.concatenate(
                [
                    wide_s[pl.ds(c * SLOTS + slot, EXPERTS, stride=period), :].astype(bf16)
                    for c in range(CHUNKS)
                ],
                axis=1,
            )
        )
    out = swiglu(jnp.concatenate(rows, axis=0), gate[0], up[0], down[0])
    size = WIDTH // CHUNKS
    for slot in range(SLOTS):
        for c in range(CHUNKS):
            wide_s[pl.ds(c * SLOTS + slot, EXPERTS, stride=period), :] = out[
                slot * EXPERTS : (slot + 1) * EXPERTS, c * size : (c + 1) * size
            ]
    back[...] = wide_s[...].astype(bf16)


def experts(arrived, gate, up, down):
    return pl.pallas_call(
        expert_kernel,
        name="experts",
        out_shape=jax.ShapeDtypeStruct(arrived.shape, bf16),
        in_specs=[vmem] * 4,
        out_specs=vmem,
        scratch_shapes=[pltpu.VMEM(arrived.shape, f32)],
        cost_estimate=pl.CostEstimate(flops=400_000_000, bytes_accessed=3_000_000, transcendentals=0),
    )(arrived, gate, up, down)


def join_kernel(a, b, c, d, o):
    n = a.shape[0]
    for i, r in enumerate((a, b, c, d)):
        o[i * n : (i + 1) * n] = r[...]


def join(pieces):
    a = pieces[0]
    return pl.pallas_call(
        join_kernel,
        name="join",
        out_shape=jax.ShapeDtypeStruct((4 * a.shape[0],) + a.shape[1:], a.dtype),
        in_specs=[vmem] * 4,
        out_specs=vmem,
    )(*pieces)


def dense_kernel(*refs):
    tokens, shards = refs[0:4], refs[4:12]
    mix, own, s_gate, s_up, s_down = refs[12:17]
    outs, shared_o = refs[17:21], refs[21]
    inputs = jnp.concatenate([t[...] for t in tokens], axis=0)
    rows = shards[0].shape[0] // 3
    gates, ups, downs = [
        jnp.concatenate([w[i * rows : (i + 1) * rows] for w in shards], axis=0) for i in range(3)
    ]
    hidden = (silu(dot_t(inputs, gates)) * dot_t(inputs, ups)).astype(bf16)
    part = dot(hidden, downs) / (1.0 + jnp.exp(-mix[...]))
    n = tokens[0].shape[0]
    for i, o in enumerate(outs):
        o[...] = part[i * n : (i + 1) * n].astype(bf16)
    shared_o[...] = swiglu(own[...], s_gate[...], s_up[...], s_down[...])


def dense(tokens, shards, mix, own, s_gate, s_up, s_down):
    part = jax.ShapeDtypeStruct(tokens[0].shape, bf16)
    outs = pl.pallas_call(
        dense_kernel,
        name="dense",
        out_shape=[part] * 4 + [jax.ShapeDtypeStruct(own.shape, f32)],
        in_specs=[vmem] * 17,
        out_specs=[vmem] * 5,
        cost_estimate=pl.CostEstimate(flops=500_000_000, bytes_accessed=5_000_000, transcendentals=0),
    )(*tokens, *shards, mix[None], own, s_gate, s_up, s_down)
    return outs[:4], outs[4]


def fold_kernel(a, b, c, d, *outs):
    total = a[...].astype(f32) + b[...].astype(f32) + c[...].astype(f32) + d[...].astype(f32)
    n = outs[0].shape[0]
    for i, o in enumerate(outs):
        o[...] = total[i * n : (i + 1) * n].astype(bf16)


def fold(pieces):
    a = pieces[0]
    return pl.pallas_call(
        fold_kernel,
        name="fold",
        out_shape=[jax.ShapeDtypeStruct((a.shape[0] // 4, a.shape[1]), bf16)] * 4,
        in_specs=[vmem] * 4,
        out_specs=[vmem] * 4,
    )(*pieces)


def final_kernel(back, combine, residual, shared, a, b, c, d, out, tall_s):
    tall_s[...] = dot(combine[...], back[...])
    routed = jnp.concatenate(
        [tall_s[pl.ds(i, SEQ, stride=CHUNKS), :] for i in range(CHUNKS)], axis=1
    )
    dense_out = a[...].astype(f32) + b[...].astype(f32) + c[...].astype(f32) + d[...].astype(f32)
    combined = shared[...] + routed + dense_out
    out[...] = (residual[...] + normed(combined)).astype(bf16)


def final(back, combine, residual, shared, pieces):
    return pl.pallas_call(
        final_kernel,
        name="final",
        out_shape=jax.ShapeDtypeStruct(residual.shape, bf16),
        in_specs=[vmem] * 8,
        out_specs=vmem,
        scratch_shapes=[pltpu.VMEM((SEQ * CHUNKS, WIDTH // CHUNKS), f32)],
    )(back, combine, residual, shared, *pieces)


def exchange(packed):
    sent = packed.reshape(EXPERTS, CHUNKS * SLOTS, WIDTH // CHUNKS)
    got = lax.all_to_all(sent, "ep", split_axis=0, concat_axis=0, tiled=True)
    return got.reshape(PACKED, WIDTH // CHUNKS)


def per_device(
    tokens,
    lengths,
    cache_keys,
    cache_values,
    retention_state,
    mix_gain,
    query_weight,
    key_weight,
    value_weight,
    out_weight,
    ffn_gain,
    routes,
    route_scores,
    expert_gate,
    expert_up,
    expert_down,
    shared_gate,
    shared_up,
    shared_down,
    dense_gate,
    dense_up,
    dense_down,
    dense_mix,
):
    residual, normal_ffn, new_keys, new_values, outgoing, combine, shard = mixer(
        tokens,
        lengths,
        mix_gain,
        ffn_gain,
        routes,
        route_scores,
        cache_keys,
        cache_values,
        retention_state,
        query_weight,
        key_weight,
        value_weight,
        out_weight,
        dense_gate,
        dense_up,
        dense_down,
    )
    arrived = exchange(outgoing)
    near = join([normal_ffn] + [flip(normal_ffn, m) for m in y_masks])
    token_pieces = [near] + [flip(near, m) for m in z_masks]
    shards = [shard] + [flip(shard, m) for m in x_masks]
    shards = shards + [flip(w, 1) for w in shards]
    back = exchange(experts(arrived, expert_gate, expert_up, expert_down))
    parts, shared_out = dense(
        token_pieces, shards, dense_mix, normal_ffn, shared_gate, shared_up, shared_down
    )
    near_parts = fold([parts[0]] + [flip(p, m) for p, m in zip(parts[1:], z_masks)])
    own_parts = [near_parts[0]] + [flip(p, m) for p, m in zip(near_parts[1:], y_masks)]
    layer_out = final(back, combine, residual, shared_out, own_parts)
    return (layer_out, new_keys, new_values)


def solution(mesh):
    in_specs = (
        P("ep", None),
        P("ep"),
        P("ep", None, None),
        P("ep", None, None),
        P("ep", None, None, None),
        P(),
        P(),
        P(),
        P(),
        P(),
        P(),
        P("ep", None),
        P("ep", None),
        P("ep", None, None),
        P("ep", None, None),
        P("ep", None, None),
        P(),
        P(),
        P(),
        P("ep", None),
        P("ep", None),
        P("ep", None),
        P(),
    )
    out_specs = (P("ep", None), P("ep", None), P("ep", None))
    return jax.shard_map(
        per_device, mesh=mesh, in_specs=in_specs, out_specs=out_specs, check_vma=False
    )
```

```python
import math

import jax
import jax.numpy as jnp
from jax import lax
from jax.experimental import pallas as pl
from jax.experimental.pallas import tpu as pltpu
from jax.sharding import PartitionSpec as P


eps = 1e-06
route_scale = 2.5
rope_base = 10000.0

SEQ = 16
WIDTH = 1024
HEADS = 4
KEY = 128
VALUE = 256
BLOCK = 128
EXPERTS = 128
SLOTS = 2
NEAR = 8
FAR = 16
HELD = SLOTS * NEAR
ROWS = FAR * HELD
GROUP = 4
MIB = 1024 * 1024

x_masks = (2, 4, 6)

f32 = jnp.float32
bf16 = jnp.bfloat16
vmem = pl.BlockSpec(memory_space=pltpu.VMEM)
hbm = pl.BlockSpec(memory_space=pltpu.HBM)


def flip(values, mask):
    return lax.ppermute(values, "ep", [(i, i ^ mask) for i in range(lax.axis_size("ep"))])


def normed(values):
    return values * lax.rsqrt(jnp.mean(values * values, axis=-1, keepdims=True) + eps)


def dot(a, b):
    return jnp.dot(a, b, preferred_element_type=f32)


def dot_t(a, b):
    return lax.dot_general(a, b, (((1,), (1,)), ((), ())), preferred_element_type=f32)


def dot_0(a, b):
    return lax.dot_general(a, b, (((0,), (0,)), ((), ())), preferred_element_type=f32)


def iota(shape, axis):
    return lax.broadcasted_iota(jnp.int32, shape, axis)


def silu(v):
    return v / (1.0 + jnp.exp(-v))


def head_rates(head_ids):
    return jnp.log1p(-jnp.exp2(-5.0 - head_ids.astype(f32)))


def rotary(length_of):
    shape = (SEQ, KEY)
    row = iota(shape, 0)
    half = KEY // 2
    position = jnp.zeros(shape, f32)
    for s in range(SEQ):
        position = jnp.where(row == s, length_of(s).astype(f32), position)
    lane = iota(shape, 1)
    inverse = jnp.exp((lane % half).astype(f32) * (-math.log(rope_base) / half))
    angles = position * inverse
    sine = jnp.sin(angles)
    return jnp.cos(angles), jnp.where(lane < half, -sine, sine)


def route_weights(routes, scores):
    expert = iota((EXPERTS, SEQ), 0)
    weight = scores / jnp.sum(scores, axis=0, keepdims=True) * route_scale
    weighted = jnp.zeros((EXPERTS, SEQ), f32)
    for k in range(routes.shape[0]):
        weighted = jnp.where(routes[k : k + 1, :] == expert, weight[k : k + 1, :], weighted)
    same = (iota((EXPERTS, EXPERTS), 0) == iota((EXPERTS, EXPERTS), 1)).astype(bf16)
    return dot_0(weighted.astype(bf16), same).astype(bf16)


def mixer_kernel(
    lengths_h,
    routes_h,
    scores_h,
    tokens_h,
    mix_gain_h,
    wq_h,
    wk_h,
    keys_h,
    wv_h,
    ffn_gain_h,
    wo_h,
    values_h,
    state_h,
    gate_h,
    up_h,
    down_h,
    residual_o,
    ffn_o,
    new_keys_o,
    new_values_o,
    outgoing_o,
    shard_o,
    lengths_s,
    routes_s,
    scores_s,
    tokens_s,
    mix_gain,
    wq,
    wk,
    keys,
    wv,
    ffn_gain,
    wo,
    values,
    state,
    weights_s,
    retained_s,
    sems,
    group_sems,
    shard_sems,
):
    sources = (
        lengths_h, routes_h, scores_h, tokens_h, mix_gain_h, wq_h, wk_h, keys_h, wv_h, ffn_gain_h, wo_h
    )
    targets = (
        lengths_s, routes_s, scores_s, tokens_s, mix_gain, wq, wk, keys, wv, ffn_gain, wo
    )
    copies = [
        pltpu.make_async_copy(src, dst, sems.at[i])
        for i, (src, dst) in enumerate(zip(sources, targets))
    ]
    steps = SEQ // GROUP
    group_copies = []
    for g in range(steps):
        part = pl.ds(g * GROUP, GROUP)
        group_copies.append(
            (
                pltpu.make_async_copy(values_h.at[part], values.at[part], group_sems.at[0, g]),
                pltpu.make_async_copy(state_h.at[part], state.at[part], group_sems.at[1, g]),
            )
        )
    for c in copies[:8]:
        c.start()
    for c in group_copies[0]:
        c.start()
    for c in copies[8:10]:
        c.start()
    for pair in group_copies[1:]:
        for c in pair:
            c.start()
    copies[10].start()
    rows = gate_h.shape[0]
    shard_copies = [
        pltpu.make_async_copy(src, shard_o.at[pl.ds(i * rows, rows)], shard_sems.at[i])
        for i, src in enumerate((gate_h, up_h, down_h))
    ]
    for c in shard_copies:
        c.start()
    for c in copies[:3]:
        c.wait()

    def filled_of(s):
        return lax.rem(lengths_s[s], BLOCK)

    route_weight = route_weights(routes_s[...], scores_s[...])

    cosine, sine = rotary(lambda s: lengths_s[s])
    cos = jnp.concatenate([cosine] * HEADS, axis=1)
    sin = jnp.concatenate([sine] * HEADS, axis=1)
    copies[3].wait()
    copies[4].wait()
    widened = tokens_s[...].astype(f32)
    normal_in = (normed(widened) * mix_gain[...]).astype(bf16)

    def rotate(raw):
        swapped = jnp.concatenate(
            [pltpu.roll(raw[:, h * KEY : (h + 1) * KEY], KEY // 2, 1) for h in range(HEADS)],
            axis=1,
        )
        return raw * cos + swapped * sin

    copies[5].wait()
    copies[6].wait()
    queries = (rotate(dot(normal_in, wq[...])) * KEY ** (-0.5)).astype(bf16)
    new_keys = rotate(dot(normal_in, wk[...])).astype(bf16)
    new_keys_o[...] = new_keys
    queries32 = queries.astype(f32)
    product = queries32 * new_keys.astype(f32)

    head_of = iota((8, HEADS * KEY), 0)
    query_block = iota((8, HEADS * KEY), 1) // KEY == head_of
    place = iota((8, BLOCK), 1)
    rate_wide = head_rates(iota((8, BLOCK), 0))
    rate_tall = head_rates(iota((8, 1), 0))
    value_block = iota((8, HEADS * VALUE), 1) // VALUE == iota((8, HEADS * VALUE), 0)

    blocked = []
    copies[7].wait()
    for s in range(SEQ):
        spread_query = jnp.where(
            query_block, jnp.broadcast_to(queries32[s : s + 1], (8, HEADS * KEY)), 0.0
        ).astype(bf16)
        blocked.append(spread_query)
        found = dot_t(spread_query, keys[s])
        distance = jnp.maximum(filled_of(s) - place, 0).astype(f32)
        weights_s[s] = jnp.where(
            place < filled_of(s), found * jnp.exp(distance * rate_wide), 0.0
        ).astype(bf16)

    for g in range(steps):
        for c in group_copies[g]:
            c.wait()
        for s in range(g * GROUP, (g + 1) * GROUP):
            inside = dot(weights_s[s], values[s])
            heads = blocked[s]
            stacked = (
                heads[:, 0:KEY]
                + heads[:, KEY : 2 * KEY]
                + heads[:, 2 * KEY : 3 * KEY]
                + heads[:, 3 * KEY : 4 * KEY]
            )
            carried = jnp.concatenate(
                [dot(stacked, state[s, h].astype(bf16)) for h in range(HEADS)], axis=1
            )
            decay = jnp.exp((filled_of(s).astype(f32) + 1.0) * rate_tall)
            both = jnp.where(value_block, inside + carried * decay, 0.0)
            retained_s[s : s + 1, :] = jnp.sum(both, axis=0, keepdims=True)

    copies[8].wait()
    copies[9].wait()
    new_values = dot(normal_in, wv[...]).astype(bf16)
    new_values_o[...] = new_values
    new_values32 = new_values.astype(f32)
    headed = []
    for h in range(HEADS):
        own = jnp.sum(product[:, h * KEY : (h + 1) * KEY], axis=1, keepdims=True)
        own = own.astype(bf16).astype(f32)
        span = slice(h * VALUE, (h + 1) * VALUE)
        headed.append(normed(retained_s[:, span] + own * new_values32[:, span]).astype(bf16))
    copies[10].wait()
    mixer_out = dot(jnp.concatenate(headed, axis=1), wo[...])
    residual = widened + normed(mixer_out)
    residual_o[...] = residual
    normal_ffn = (normed(residual) * ffn_gain[...]).astype(bf16)
    ffn_o[...] = normal_ffn
    row = jnp.concatenate([normal_ffn, route_weight], axis=1)
    outgoing_o[...] = jnp.broadcast_to(row[None], outgoing_o.shape)
    for c in shard_copies:
        c.wait()


def mixer(
    tokens, lengths, mix_gain, ffn_gain, routes, scores, cache_keys, cache_values, state, wq, wk, wv, wo, gate, up, down
):
    shapes = [
        jax.ShapeDtypeStruct((SEQ, WIDTH), f32),
        jax.ShapeDtypeStruct((SEQ, WIDTH), bf16),
        jax.ShapeDtypeStruct((SEQ, HEADS * KEY), bf16),
        jax.ShapeDtypeStruct((SEQ, WIDTH), bf16),
        jax.ShapeDtypeStruct((NEAR, SEQ, WIDTH + EXPERTS), bf16),
        jax.ShapeDtypeStruct((3 * gate.shape[0], WIDTH), bf16),
    ]
    held = (
        routes.T, scores.T, tokens, mix_gain[None], wq, wk, cache_keys, wv, ffn_gain[None], wo, cache_values, state
    )
    return pl.pallas_call(
        mixer_kernel,
        name="mixer",
        out_shape=shapes,
        in_specs=[hbm] * 16,
        out_specs=[vmem] * 5 + [hbm],
        scratch_shapes=[pltpu.SMEM((SEQ,), jnp.int32)]
        + [pltpu.VMEM(a.shape, a.dtype) for a in held]
        + [
            pltpu.VMEM((SEQ, 8, BLOCK), bf16),
            pltpu.VMEM((SEQ, WIDTH), f32),
            pltpu.SemaphoreType.DMA((11,)),
            pltpu.SemaphoreType.DMA((2, SEQ // GROUP)),
            pltpu.SemaphoreType.DMA((3,)),
        ],
        cost_estimate=pl.CostEstimate(flops=2_000_000_000, bytes_accessed=22_000_000, transcendentals=0),
        compiler_params=pltpu.CompilerParams(vmem_limit_bytes=60 * MIB),
    )(lengths, *held, gate, up, down)


def swiglu(inputs, w_gate, w_up, w_down):
    hidden = (silu(dot(inputs, w_gate)) * dot(inputs, w_up)).astype(bf16)
    return dot(hidden, w_down)


def select_kernel(index, near, own, outgoing_o, combine_o):
    tokens = near[:, :, 0:WIDTH].reshape(NEAR * SEQ, WIDTH)
    weights = near[:, :, WIDTH:].reshape(NEAR * SEQ, EXPERTS)
    expert = iota((EXPERTS, ROWS), 1) // HELD * NEAR + index[0]
    pick = (iota((EXPERTS, ROWS), 0) == expert).astype(bf16)
    weight = dot(weights, pick)
    named = (weight > 0.0).astype(bf16)
    shape = (NEAR * SEQ, NEAR * SEQ)
    earlier = (iota(shape, 1) < iota(shape, 0)).astype(bf16)
    rank = dot(earlier, named)
    slot = (iota((NEAR * SEQ, ROWS), 1) % HELD).astype(f32)
    combine = jnp.where(rank == slot, weight, 0.0)
    combine_o[...] = combine.astype(bf16)
    chosen = dot_0((combine > 0.0).astype(bf16), tokens).astype(bf16)
    outgoing_o[:, 0:HELD, :] = chosen.reshape(FAR, HELD, WIDTH)
    outgoing_o[:, HELD:, :] = jnp.broadcast_to(own[...][None], (FAR, SEQ, WIDTH))


def select(index, near, own):
    return pl.pallas_call(
        select_kernel,
        name="select",
        out_shape=[
            jax.ShapeDtypeStruct((FAR, HELD + SEQ, WIDTH), bf16),
            jax.ShapeDtypeStruct((NEAR * SEQ, ROWS), bf16),
        ],
        in_specs=[pl.BlockSpec(memory_space=pltpu.SMEM)] + [vmem] * 2,
        out_specs=[vmem] * 2,
        compiler_params=pltpu.CompilerParams(vmem_limit_bytes=12 * MIB),
    )(index, near, own)


def swiglu(inputs, w_gate, w_up, w_down):
    hidden = (silu(dot(inputs, w_gate)) * dot(inputs, w_up)).astype(bf16)
    return dot(hidden, w_down)


def expert_kernel(*refs):
    arrived, gate, up, down, mix = refs[0:5]
    shards, back = refs[5:13], refs[13]
    rows = arrived[:, 0:HELD, :].reshape(ROWS, WIDTH)
    out = swiglu(rows, gate[0], up[0], down[0]).astype(bf16)
    back[:, 0:HELD, :] = out.reshape(FAR, HELD, WIDTH)
    tokens = arrived[:, HELD:, :].reshape(FAR * SEQ, WIDTH)
    n = shards[0].shape[0] // 3
    gates, ups, downs = [
        jnp.concatenate([w[i * n : (i + 1) * n] for w in shards], axis=0) for i in range(3)
    ]
    hidden = (silu(dot_t(tokens, gates)) * dot_t(tokens, ups)).astype(bf16)
    part = dot(hidden, downs) / (1.0 + jnp.exp(-mix[...]))
    back[:, HELD:, :] = part.astype(bf16).reshape(FAR, SEQ, WIDTH)


def experts(arrived, gate, up, down, mix, shards):
    return pl.pallas_call(
        expert_kernel,
        name="experts",
        out_shape=jax.ShapeDtypeStruct(arrived.shape, bf16),
        in_specs=[vmem] * 13,
        out_specs=vmem,
        cost_estimate=pl.CostEstimate(flops=900_000_000, bytes_accessed=6_000_000, transcendentals=0),
        compiler_params=pltpu.CompilerParams(vmem_limit_bytes=24 * MIB),
    )(arrived, gate, up, down, mix[None], *shards)


def combine_kernel(back, combine, parts_o):
    rows = back[:, 0:HELD, :].reshape(ROWS, WIDTH)
    parts_o[...] = dot(combine[...], rows).astype(bf16).reshape(NEAR, SEQ, WIDTH)


def combine_near(back, combine):
    return pl.pallas_call(
        combine_kernel,
        name="combine",
        out_shape=jax.ShapeDtypeStruct((NEAR, SEQ, WIDTH), bf16),
        in_specs=[vmem] * 2,
        out_specs=vmem,
        compiler_params=pltpu.CompilerParams(vmem_limit_bytes=8 * MIB),
    )(back, combine)


def local_kernel(back, own, s_gate, s_up, s_down, out):
    out[...] = swiglu(own[...], s_gate[...], s_up[...], s_down[...]) + jnp.sum(
        back[:, HELD:, :].astype(f32), axis=0
    )


def local(back, own, s_gate, s_up, s_down):
    return pl.pallas_call(
        local_kernel,
        name="local",
        out_shape=jax.ShapeDtypeStruct((SEQ, WIDTH), f32),
        in_specs=[vmem] * 5,
        out_specs=vmem,
        cost_estimate=pl.CostEstimate(flops=900_000_000, bytes_accessed=2_000_000, transcendentals=0),
        compiler_params=pltpu.CompilerParams(vmem_limit_bytes=8 * MIB),
    )(back, own, s_gate, s_up, s_down)


def final_kernel(parts, residual, extra, out):
    combined = extra[...] + jnp.sum(parts[...].astype(f32), axis=0)
    out[...] = (residual[...] + normed(combined)).astype(bf16)


def final(parts, residual, extra):
    return pl.pallas_call(
        final_kernel,
        name="final",
        out_shape=jax.ShapeDtypeStruct(residual.shape, bf16),
        in_specs=[vmem] * 3,
        out_specs=vmem,
        compiler_params=pltpu.CompilerParams(vmem_limit_bytes=4 * MIB),
    )(parts, residual, extra)


near_groups = [[NEAR * p + j for j in range(NEAR)] for p in range(FAR)]
far_groups = [[NEAR * p + j for p in range(FAR)] for j in range(NEAR)]


def exchange(values, groups):
    return lax.all_to_all(
        values, "ep", split_axis=0, concat_axis=0, axis_index_groups=groups, tiled=True
    )


def per_device(
    tokens,
    lengths,
    cache_keys,
    cache_values,
    retention_state,
    mix_gain,
    query_weight,
    key_weight,
    value_weight,
    out_weight,
    ffn_gain,
    routes,
    route_scores,
    expert_gate,
    expert_up,
    expert_down,
    shared_gate,
    shared_up,
    shared_down,
    dense_gate,
    dense_up,
    dense_down,
    dense_mix,
):
    residual, normal_ffn, new_keys, new_values, outgoing, shard = mixer(
        tokens,
        lengths,
        mix_gain,
        ffn_gain,
        routes,
        route_scores,
        cache_keys,
        cache_values,
        retention_state,
        query_weight,
        key_weight,
        value_weight,
        out_weight,
        dense_gate,
        dense_up,
        dense_down,
    )
    near = exchange(outgoing, near_groups)
    shards = [shard] + [flip(shard, m) for m in x_masks]
    shards = shards + [flip(w, 1) for w in shards]
    index = (lax.axis_index("ep") % NEAR).astype(jnp.int32)[None]
    chosen, combine = select(index, near, normal_ffn)
    arrived = exchange(chosen, far_groups)
    back = exchange(
        experts(arrived, expert_gate, expert_up, expert_down, dense_mix, shards), far_groups
    )
    parts = exchange(combine_near(back, combine), near_groups)
    extra = local(back, normal_ffn, shared_gate, shared_up, shared_down)
    layer_out = final(parts, residual, extra)
    return (layer_out, new_keys, new_values)


def solution(mesh):
    in_specs = (
        P("ep", None),
        P("ep"),
        P("ep", None, None),
        P("ep", None, None),
        P("ep", None, None, None),
        P(),
        P(),
        P(),
        P(),
        P(),
        P(),
        P("ep", None),
        P("ep", None),
        P("ep", None, None),
        P("ep", None, None),
        P("ep", None, None),
        P(),
        P(),
        P(),
        P("ep", None),
        P("ep", None),
        P("ep", None),
        P(),
    )
    out_specs = (P("ep", None), P("ep", None), P("ep", None))
    return jax.shard_map(
        per_device, mesh=mesh, in_specs=in_specs, out_specs=out_specs, check_vma=False
    )
```

```python
import math

import jax
import jax.numpy as jnp
from jax import lax
from jax.experimental import pallas as pl
from jax.experimental.pallas import tpu as pltpu
from jax.sharding import PartitionSpec as P


eps = 1e-06
route_scale = 2.5
rope_base = 10000.0

SEQ = 16
WIDTH = 1024
HEADS = 4
KEY = 128
VALUE = 256
BLOCK = 128
EXPERTS = 128
SLOTS = 2
NEAR = 8
FAR = 16
HELD = SLOTS * NEAR
ROWS = FAR * HELD
GROUP = 4
MIB = 1024 * 1024

near_masks = (6, 24, 96)
far_masks = (1, 2, 8, 32)
gate_masks = (32, 8, 2)
up_masks = (8, 2, 32)
down_masks = (2, 32, 8)

f32 = jnp.float32
bf16 = jnp.bfloat16
vmem = pl.BlockSpec(memory_space=pltpu.VMEM)
hbm = pl.BlockSpec(memory_space=pltpu.HBM)


def flip(values, mask):
    return lax.ppermute(values, "ep", [(i, i ^ mask) for i in range(lax.axis_size("ep"))])


def normed(values):
    return values * lax.rsqrt(jnp.mean(values * values, axis=-1, keepdims=True) + eps)


def dot(a, b):
    return jnp.dot(a, b, preferred_element_type=f32)


def dot_t(a, b):
    return lax.dot_general(a, b, (((1,), (1,)), ((), ())), preferred_element_type=f32)


def dot_0(a, b):
    return lax.dot_general(a, b, (((0,), (0,)), ((), ())), preferred_element_type=f32)


def iota(shape, axis):
    return lax.broadcasted_iota(jnp.int32, shape, axis)


def silu(v):
    return v / (1.0 + jnp.exp(-v))


def head_rates(head_ids):
    return jnp.log1p(-jnp.exp2(-5.0 - head_ids.astype(f32)))


def rotary(length_of):
    shape = (SEQ, KEY)
    row = iota(shape, 0)
    half = KEY // 2
    position = jnp.zeros(shape, f32)
    for s in range(SEQ):
        position = jnp.where(row == s, length_of(s).astype(f32), position)
    lane = iota(shape, 1)
    inverse = jnp.exp((lane % half).astype(f32) * (-math.log(rope_base) / half))
    angles = position * inverse
    sine = jnp.sin(angles)
    return jnp.cos(angles), jnp.where(lane < half, -sine, sine)


def route_weights(routes, scores):
    expert = iota((EXPERTS, SEQ), 0)
    weight = scores / jnp.sum(scores, axis=0, keepdims=True) * route_scale
    weighted = jnp.zeros((EXPERTS, SEQ), f32)
    for k in range(routes.shape[0]):
        weighted = jnp.where(routes[k : k + 1, :] == expert, weight[k : k + 1, :], weighted)
    same = (iota((EXPERTS, EXPERTS), 0) == iota((EXPERTS, EXPERTS), 1)).astype(bf16)
    return dot_0(weighted.astype(bf16), same).astype(bf16)


def mixer_kernel(
    lengths_h,
    routes_h,
    scores_h,
    tokens_h,
    mix_gain_h,
    wq_h,
    wk_h,
    keys_h,
    wv_h,
    ffn_gain_h,
    wo_h,
    values_h,
    state_h,
    residual_o,
    ffn_o,
    new_keys_o,
    new_values_o,
    outgoing_o,
    lengths_s,
    routes_s,
    scores_s,
    tokens_s,
    mix_gain,
    wq,
    wk,
    keys,
    wv,
    ffn_gain,
    wo,
    values,
    state,
    weights_s,
    retained_s,
    sems,
    group_sems,
):
    sources = (
        lengths_h, routes_h, scores_h, tokens_h, mix_gain_h, wq_h, wk_h, keys_h, wv_h, ffn_gain_h, wo_h
    )
    targets = (
        lengths_s, routes_s, scores_s, tokens_s, mix_gain, wq, wk, keys, wv, ffn_gain, wo
    )
    copies = [
        pltpu.make_async_copy(src, dst, sems.at[i])
        for i, (src, dst) in enumerate(zip(sources, targets))
    ]
    steps = SEQ // GROUP
    group_copies = []
    for g in range(steps):
        part = pl.ds(g * GROUP, GROUP)
        group_copies.append(
            (
                pltpu.make_async_copy(values_h.at[part], values.at[part], group_sems.at[0, g]),
                pltpu.make_async_copy(state_h.at[part], state.at[part], group_sems.at[1, g]),
            )
        )
    for c in copies[:8]:
        c.start()
    for c in group_copies[0]:
        c.start()
    for c in copies[8:10]:
        c.start()
    for pair in group_copies[1:]:
        for c in pair:
            c.start()
    copies[10].start()
    for c in copies[:3]:
        c.wait()

    def filled_of(s):
        return lax.rem(lengths_s[s], BLOCK)

    route_weight = route_weights(routes_s[...], scores_s[...])

    cosine, sine = rotary(lambda s: lengths_s[s])
    cos = jnp.concatenate([cosine] * HEADS, axis=1)
    sin = jnp.concatenate([sine] * HEADS, axis=1)
    copies[3].wait()
    copies[4].wait()
    widened = tokens_s[...].astype(f32)
    normal_in = (normed(widened) * mix_gain[...]).astype(bf16)

    def rotate(raw):
        swapped = jnp.concatenate(
            [pltpu.roll(raw[:, h * KEY : (h + 1) * KEY], KEY // 2, 1) for h in range(HEADS)],
            axis=1,
        )
        return raw * cos + swapped * sin

    copies[5].wait()
    copies[6].wait()
    queries = (rotate(dot(normal_in, wq[...])) * KEY ** (-0.5)).astype(bf16)
    new_keys = rotate(dot(normal_in, wk[...])).astype(bf16)
    new_keys_o[...] = new_keys
    queries32 = queries.astype(f32)
    product = queries32 * new_keys.astype(f32)

    head_of = iota((8, HEADS * KEY), 0)
    query_block = iota((8, HEADS * KEY), 1) // KEY == head_of
    place = iota((8, BLOCK), 1)
    rate_wide = head_rates(iota((8, BLOCK), 0))
    rate_tall = head_rates(iota((8, 1), 0))
    value_block = iota((8, HEADS * VALUE), 1) // VALUE == iota((8, HEADS * VALUE), 0)

    blocked = []
    copies[7].wait()
    for s in range(SEQ):
        spread_query = jnp.where(
            query_block, jnp.broadcast_to(queries32[s : s + 1], (8, HEADS * KEY)), 0.0
        ).astype(bf16)
        blocked.append(spread_query)
        found = dot_t(spread_query, keys[s])
        distance = jnp.maximum(filled_of(s) - place, 0).astype(f32)
        weights_s[s] = jnp.where(
            place < filled_of(s), found * jnp.exp(distance * rate_wide), 0.0
        ).astype(bf16)

    for g in range(steps):
        for c in group_copies[g]:
            c.wait()
        for s in range(g * GROUP, (g + 1) * GROUP):
            inside = dot(weights_s[s], values[s])
            heads = blocked[s]
            stacked = (
                heads[:, 0:KEY]
                + heads[:, KEY : 2 * KEY]
                + heads[:, 2 * KEY : 3 * KEY]
                + heads[:, 3 * KEY : 4 * KEY]
            )
            carried = jnp.concatenate(
                [dot(stacked, state[s, h].astype(bf16)) for h in range(HEADS)], axis=1
            )
            decay = jnp.exp((filled_of(s).astype(f32) + 1.0) * rate_tall)
            both = jnp.where(value_block, inside + carried * decay, 0.0)
            retained_s[s : s + 1, :] = jnp.sum(both, axis=0, keepdims=True)

    copies[8].wait()
    copies[9].wait()
    new_values = dot(normal_in, wv[...]).astype(bf16)
    new_values_o[...] = new_values
    new_values32 = new_values.astype(f32)
    headed = []
    for h in range(HEADS):
        own = jnp.sum(product[:, h * KEY : (h + 1) * KEY], axis=1, keepdims=True)
        own = own.astype(bf16).astype(f32)
        span = slice(h * VALUE, (h + 1) * VALUE)
        headed.append(normed(retained_s[:, span] + own * new_values32[:, span]).astype(bf16))
    copies[10].wait()
    mixer_out = dot(jnp.concatenate(headed, axis=1), wo[...])
    residual = widened + normed(mixer_out)
    residual_o[...] = residual
    normal_ffn = (normed(residual) * ffn_gain[...]).astype(bf16)
    ffn_o[...] = normal_ffn
    row = jnp.concatenate([normal_ffn, route_weight], axis=1)
    outgoing_o[...] = jnp.broadcast_to(row[None], outgoing_o.shape)


def mixer(
    tokens, lengths, mix_gain, ffn_gain, routes, scores, cache_keys, cache_values, state, wq, wk, wv, wo
):
    shapes = [
        jax.ShapeDtypeStruct((SEQ, WIDTH), f32),
        jax.ShapeDtypeStruct((SEQ, WIDTH), bf16),
        jax.ShapeDtypeStruct((SEQ, HEADS * KEY), bf16),
        jax.ShapeDtypeStruct((SEQ, WIDTH), bf16),
        jax.ShapeDtypeStruct((NEAR, SEQ, WIDTH + EXPERTS), bf16),
    ]
    held = (
        routes.T, scores.T, tokens, mix_gain[None], wq, wk, cache_keys, wv, ffn_gain[None], wo, cache_values, state
    )
    return pl.pallas_call(
        mixer_kernel,
        name="mixer",
        out_shape=shapes,
        in_specs=[hbm] * 13,
        out_specs=[vmem] * 5,
        scratch_shapes=[pltpu.SMEM((SEQ,), jnp.int32)]
        + [pltpu.VMEM(a.shape, a.dtype) for a in held]
        + [
            pltpu.VMEM((SEQ, 8, BLOCK), bf16),
            pltpu.VMEM((SEQ, WIDTH), f32),
            pltpu.SemaphoreType.DMA((11,)),
            pltpu.SemaphoreType.DMA((2, SEQ // GROUP)),
        ],
        cost_estimate=pl.CostEstimate(flops=2_000_000_000, bytes_accessed=22_000_000, transcendentals=0),
        compiler_params=pltpu.CompilerParams(vmem_limit_bytes=60 * MIB),
    )(lengths, *held)


def swiglu(inputs, w_gate, w_up, w_down):
    hidden = (silu(dot(inputs, w_gate)) * dot(inputs, w_up)).astype(bf16)
    return dot(hidden, w_down)


def mixed(bits, masks):
    total = jnp.zeros_like(bits)
    for i, mask in enumerate(masks):
        total = total | (((bits >> i) & 1) * mask)
    return total


def select_kernel(index, near, outgoing_o, combine_o):
    tokens = near[:, :, 0:WIDTH].reshape(NEAR * SEQ, WIDTH)
    weights = near[:, :, WIDTH:].reshape(NEAR * SEQ, EXPERTS)
    expert = mixed(iota((EXPERTS, ROWS), 1) // HELD, far_masks) ^ index[0]
    pick = (iota((EXPERTS, ROWS), 0) == expert).astype(bf16)
    weight = dot(weights, pick)
    named = (weight > 0.0).astype(bf16)
    shape = (NEAR * SEQ, NEAR * SEQ)
    earlier = (iota(shape, 1) < iota(shape, 0)).astype(bf16)
    rank = dot(earlier, named)
    slot = (iota((NEAR * SEQ, ROWS), 1) % HELD).astype(f32)
    combine = jnp.where(rank == slot, weight, 0.0)
    combine_o[...] = combine.astype(bf16)
    chosen = dot_0((combine > 0.0).astype(bf16), tokens).astype(bf16)
    outgoing_o[...] = chosen.reshape(FAR, HELD, WIDTH)


def select(index, near):
    return pl.pallas_call(
        select_kernel,
        name="select",
        out_shape=[
            jax.ShapeDtypeStruct((FAR, HELD, WIDTH), bf16),
            jax.ShapeDtypeStruct((NEAR * SEQ, ROWS), bf16),
        ],
        in_specs=[pl.BlockSpec(memory_space=pltpu.SMEM), vmem],
        out_specs=[vmem] * 2,
        compiler_params=pltpu.CompilerParams(vmem_limit_bytes=8 * MIB),
    )(index, near)


def swiglu(inputs, w_gate, w_up, w_down):
    hidden = (silu(dot(inputs, w_gate)) * dot(inputs, w_up)).astype(bf16)
    return dot(hidden, w_down)


def expert_kernel(arrived, gate, up, down, back):
    rows = arrived[...].reshape(ROWS, WIDTH)
    out = swiglu(rows, gate[0], up[0], down[0]).astype(bf16)
    back[...] = out.reshape(FAR, HELD, WIDTH)


def experts(arrived, gate, up, down):
    return pl.pallas_call(
        expert_kernel,
        name="experts",
        out_shape=jax.ShapeDtypeStruct(arrived.shape, bf16),
        in_specs=[vmem] * 4,
        out_specs=vmem,
        cost_estimate=pl.CostEstimate(flops=500_000_000, bytes_accessed=3_000_000, transcendentals=0),
        compiler_params=pltpu.CompilerParams(vmem_limit_bytes=8 * MIB),
    )(arrived, gate, up, down)


def join_kernel(a0, a1, b0, b1, c0, c1, a, b, c):
    n = a0.shape[0]
    for first, second, out in ((a0, a1, a), (b0, b1, b), (c0, c1, c)):
        out[0:n] = first[...]
        out[n:] = second[...]


def join(pairs):
    rows, width = pairs[0][0].shape
    return pl.pallas_call(
        join_kernel,
        name="join",
        out_shape=[jax.ShapeDtypeStruct((2 * rows, width), bf16)] * 3,
        in_specs=[vmem] * 6,
        out_specs=[vmem] * 3,
        compiler_params=pltpu.CompilerParams(vmem_limit_bytes=4 * MIB),
    )(*[w for pair in pairs for w in pair])


def offsets(masks):
    found = [0]
    for m in masks:
        found = found + [f ^ m for f in found]
    return found


def dense_kernel(near, other, g0, g1, u0, u1, d0, d1, mix, own_o, other_o):
    count = NEAR * SEQ
    inputs = jnp.concatenate(
        [t[:, :, 0:WIDTH].reshape(count, WIDTH) for t in (near, other)], axis=0
    )
    order = offsets(gate_masks)
    n = 2 * g0.shape[0] // len(order)

    def ordered(first, second, masks):
        have = offsets(masks)
        half = len(have) // 2
        blocks = []
        for o in order:
            k = have.index(o)
            ref = first if k < half else second
            k = k % half
            blocks.append(ref[k * n : (k + 1) * n])
        return jnp.concatenate(blocks, axis=0)

    gates = ordered(g0, g1, gate_masks)
    ups = ordered(u0, u1, up_masks)
    downs = ordered(d0, d1, down_masks)
    hidden = (silu(dot_t(inputs, gates)) * dot_t(inputs, ups)).astype(bf16)
    part = (dot(hidden, downs) / (1.0 + jnp.exp(-mix[...]))).astype(bf16)
    own_o[...] = part[0:count].reshape(NEAR, SEQ, WIDTH)
    other_o[...] = part[count:].reshape(NEAR, SEQ, WIDTH)


def dense(near, other, weights, mix):
    part = jax.ShapeDtypeStruct((NEAR, SEQ, WIDTH), bf16)
    return pl.pallas_call(
        dense_kernel,
        name="dense",
        out_shape=[part] * 2,
        in_specs=[vmem] * 9,
        out_specs=[vmem] * 2,
        cost_estimate=pl.CostEstimate(flops=500_000_000, bytes_accessed=4_000_000, transcendentals=0),
        compiler_params=pltpu.CompilerParams(vmem_limit_bytes=12 * MIB),
    )(near, other, *weights, mix[None])


def combine_kernel(back, combine, own, other, parts_o):
    rows = back[...].reshape(ROWS, WIDTH)
    total = dot(combine[...], rows).reshape(NEAR, SEQ, WIDTH)
    parts_o[...] = (total + own[...].astype(f32) + other[...].astype(f32)).astype(bf16)


def combine_near(back, combine, own, other):
    return pl.pallas_call(
        combine_kernel,
        name="combine",
        out_shape=jax.ShapeDtypeStruct((NEAR, SEQ, WIDTH), bf16),
        in_specs=[vmem] * 4,
        out_specs=vmem,
        compiler_params=pltpu.CompilerParams(vmem_limit_bytes=8 * MIB),
    )(back, combine, own, other)


def shared_kernel(own, s_gate, s_up, s_down, out):
    out[...] = swiglu(own[...], s_gate[...], s_up[...], s_down[...])


def shared(own, s_gate, s_up, s_down):
    return pl.pallas_call(
        shared_kernel,
        name="shared",
        out_shape=jax.ShapeDtypeStruct((SEQ, WIDTH), f32),
        in_specs=[vmem] * 4,
        out_specs=vmem,
        cost_estimate=pl.CostEstimate(flops=900_000_000, bytes_accessed=2_000_000, transcendentals=0),
        compiler_params=pltpu.CompilerParams(vmem_limit_bytes=4 * MIB),
    )(own, s_gate, s_up, s_down)


def final_kernel(parts, residual, extra, out):
    combined = extra[...] + jnp.sum(parts[...].astype(f32), axis=0)
    out[...] = (residual[...] + normed(combined)).astype(bf16)


def final(parts, residual, extra):
    return pl.pallas_call(
        final_kernel,
        name="final",
        out_shape=jax.ShapeDtypeStruct(residual.shape, bf16),
        in_specs=[vmem] * 3,
        out_specs=vmem,
        compiler_params=pltpu.CompilerParams(vmem_limit_bytes=4 * MIB),
    )(parts, residual, extra)


near_groups = [[r ^ f for r in offsets(near_masks)] for f in offsets(far_masks)]
far_groups = [[r ^ f for f in offsets(far_masks)] for r in offsets(near_masks)]


def exchange(values, groups):
    return lax.all_to_all(
        values, "ep", split_axis=0, concat_axis=0, axis_index_groups=groups, tiled=True
    )


def per_device(
    tokens,
    lengths,
    cache_keys,
    cache_values,
    retention_state,
    mix_gain,
    query_weight,
    key_weight,
    value_weight,
    out_weight,
    ffn_gain,
    routes,
    route_scores,
    expert_gate,
    expert_up,
    expert_down,
    shared_gate,
    shared_up,
    shared_down,
    dense_gate,
    dense_up,
    dense_down,
    dense_mix,
):
    residual, normal_ffn, new_keys, new_values, outgoing = mixer(
        tokens,
        lengths,
        mix_gain,
        ffn_gain,
        routes,
        route_scores,
        cache_keys,
        cache_values,
        retention_state,
        query_weight,
        key_weight,
        value_weight,
        out_weight,
    )
    near = exchange(outgoing, near_groups)
    place = lax.axis_index("ep").astype(jnp.int32)
    index = mixed((place >> 2) & 1 | (place >> 3) & 2 | (place >> 4) & 4, near_masks)
    chosen, combine = select(index[None], near)

    masks = (gate_masks, up_masks, down_masks)
    held = [dense_gate, dense_up, dense_down]
    for stage in range(2):
        held = join([(w, flip(w, m[stage])) for w, m in zip(held, masks)])
    weights = []
    for w, m in zip(held, masks):
        weights += [w, flip(w, m[2])]
    own_part, other_part = dense(near, flip(near, 1), weights, dense_mix)

    arrived = exchange(chosen, far_groups)
    back = exchange(experts(arrived, expert_gate, expert_up, expert_down), far_groups)
    parts = exchange(combine_near(back, combine, own_part, flip(other_part, 1)), near_groups)
    extra = shared(normal_ffn, shared_gate, shared_up, shared_down)
    layer_out = final(parts, residual, extra)
    return (layer_out, new_keys, new_values)


def solution(mesh):
    in_specs = (
        P("ep", None),
        P("ep"),
        P("ep", None, None),
        P("ep", None, None),
        P("ep", None, None, None),
        P(),
        P(),
        P(),
        P(),
        P(),
        P(),
        P("ep", None),
        P("ep", None),
        P("ep", None, None),
        P("ep", None, None),
        P("ep", None, None),
        P(),
        P(),
        P(),
        P("ep", None),
        P("ep", None),
        P("ep", None),
        P(),
    )
    out_specs = (P("ep", None), P("ep", None), P("ep", None))
    return jax.shard_map(
        per_device, mesh=mesh, in_specs=in_specs, out_specs=out_specs, check_vma=False
    )
```

```python
import math

import jax
import jax.numpy as jnp
from jax import lax
from jax.experimental import pallas as pl
from jax.experimental.pallas import tpu as pltpu
from jax.sharding import PartitionSpec as P


eps = 1e-06
route_scale = 2.5
rope_base = 10000.0

SEQ = 16
WIDTH = 1024
HEADS = 4
KEY = 128
VALUE = 256
BLOCK = 128
EXPERTS = 128
SLOTS = 2
NEAR = 8
FAR = 16
HELD = SLOTS * NEAR
ROWS = FAR * HELD
GROUP = 4
MIB = 1024 * 1024

near_masks = (6, 24, 96)
far_masks = (1, 2, 8, 32)

f32 = jnp.float32
bf16 = jnp.bfloat16
vmem = pl.BlockSpec(memory_space=pltpu.VMEM)
hbm = pl.BlockSpec(memory_space=pltpu.HBM)


def flip(values, mask):
    return lax.ppermute(values, "ep", [(i, i ^ mask) for i in range(lax.axis_size("ep"))])


def normed(values):
    return values * lax.rsqrt(jnp.mean(values * values, axis=-1, keepdims=True) + eps)


def dot(a, b):
    return jnp.dot(a, b, preferred_element_type=f32)


def dot_t(a, b):
    return lax.dot_general(a, b, (((1,), (1,)), ((), ())), preferred_element_type=f32)


def dot_0(a, b):
    return lax.dot_general(a, b, (((0,), (0,)), ((), ())), preferred_element_type=f32)


def iota(shape, axis):
    return lax.broadcasted_iota(jnp.int32, shape, axis)


def silu(v):
    return v / (1.0 + jnp.exp(-v))


def head_rates(head_ids):
    return jnp.log1p(-jnp.exp2(-5.0 - head_ids.astype(f32)))


def rotary(length_of):
    shape = (SEQ, KEY)
    row = iota(shape, 0)
    half = KEY // 2
    position = jnp.zeros(shape, f32)
    for s in range(SEQ):
        position = jnp.where(row == s, length_of(s).astype(f32), position)
    lane = iota(shape, 1)
    inverse = jnp.exp((lane % half).astype(f32) * (-math.log(rope_base) / half))
    angles = position * inverse
    sine = jnp.sin(angles)
    return jnp.cos(angles), jnp.where(lane < half, -sine, sine)


def route_weights(routes, scores):
    expert = iota((EXPERTS, SEQ), 0)
    weight = scores / jnp.sum(scores, axis=0, keepdims=True) * route_scale
    weighted = jnp.zeros((EXPERTS, SEQ), f32)
    for k in range(routes.shape[0]):
        weighted = jnp.where(routes[k : k + 1, :] == expert, weight[k : k + 1, :], weighted)
    same = (iota((EXPERTS, EXPERTS), 0) == iota((EXPERTS, EXPERTS), 1)).astype(bf16)
    return dot_0(weighted.astype(bf16), same).astype(bf16)


def mixer_kernel(
    lengths_h,
    routes_h,
    scores_h,
    tokens_h,
    mix_gain_h,
    wq_h,
    wk_h,
    keys_h,
    wv_h,
    ffn_gain_h,
    wo_h,
    values_h,
    state_h,
    gate_h,
    up_h,
    down_h,
    residual_o,
    ffn_o,
    new_keys_o,
    new_values_o,
    outgoing_o,
    shard_o,
    lengths_s,
    routes_s,
    scores_s,
    tokens_s,
    mix_gain,
    wq,
    wk,
    keys,
    wv,
    ffn_gain,
    wo,
    values,
    state,
    weights_s,
    retained_s,
    sems,
    group_sems,
    shard_sems,
):
    sources = (
        lengths_h, routes_h, scores_h, tokens_h, mix_gain_h, wq_h, wk_h, keys_h, wv_h, ffn_gain_h, wo_h
    )
    targets = (
        lengths_s, routes_s, scores_s, tokens_s, mix_gain, wq, wk, keys, wv, ffn_gain, wo
    )
    copies = [
        pltpu.make_async_copy(src, dst, sems.at[i])
        for i, (src, dst) in enumerate(zip(sources, targets))
    ]
    steps = SEQ // GROUP
    group_copies = []
    for g in range(steps):
        part = pl.ds(g * GROUP, GROUP)
        group_copies.append(
            (
                pltpu.make_async_copy(values_h.at[part], values.at[part], group_sems.at[0, g]),
                pltpu.make_async_copy(state_h.at[part], state.at[part], group_sems.at[1, g]),
            )
        )
    for c in copies[:8]:
        c.start()
    for c in group_copies[0]:
        c.start()
    for c in copies[8:10]:
        c.start()
    for pair in group_copies[1:]:
        for c in pair:
            c.start()
    copies[10].start()
    rows = gate_h.shape[0]
    shard_copies = [
        pltpu.make_async_copy(src, shard_o.at[pl.ds(i * rows, rows)], shard_sems.at[i])
        for i, src in enumerate((gate_h, up_h, down_h))
    ]
    for c in shard_copies:
        c.start()
    for c in copies[:3]:
        c.wait()

    def filled_of(s):
        return lax.rem(lengths_s[s], BLOCK)

    route_weight = route_weights(routes_s[...], scores_s[...])

    cosine, sine = rotary(lambda s: lengths_s[s])
    cos = jnp.concatenate([cosine] * HEADS, axis=1)
    sin = jnp.concatenate([sine] * HEADS, axis=1)
    copies[3].wait()
    copies[4].wait()
    widened = tokens_s[...].astype(f32)
    normal_in = (normed(widened) * mix_gain[...]).astype(bf16)

    def rotate(raw):
        swapped = jnp.concatenate(
            [pltpu.roll(raw[:, h * KEY : (h + 1) * KEY], KEY // 2, 1) for h in range(HEADS)],
            axis=1,
        )
        return raw * cos + swapped * sin

    copies[5].wait()
    copies[6].wait()
    queries = (rotate(dot(normal_in, wq[...])) * KEY ** (-0.5)).astype(bf16)
    new_keys = rotate(dot(normal_in, wk[...])).astype(bf16)
    new_keys_o[...] = new_keys
    queries32 = queries.astype(f32)
    product = queries32 * new_keys.astype(f32)

    head_of = iota((8, HEADS * KEY), 0)
    query_block = iota((8, HEADS * KEY), 1) // KEY == head_of
    place = iota((8, BLOCK), 1)
    rate_wide = head_rates(iota((8, BLOCK), 0))
    rate_tall = head_rates(iota((8, 1), 0))
    value_block = iota((8, HEADS * VALUE), 1) // VALUE == iota((8, HEADS * VALUE), 0)

    blocked = []
    copies[7].wait()
    for s in range(SEQ):
        spread_query = jnp.where(
            query_block, jnp.broadcast_to(queries32[s : s + 1], (8, HEADS * KEY)), 0.0
        ).astype(bf16)
        blocked.append(spread_query)
        found = dot_t(spread_query, keys[s])
        distance = jnp.maximum(filled_of(s) - place, 0).astype(f32)
        weights_s[s] = jnp.where(
            place < filled_of(s), found * jnp.exp(distance * rate_wide), 0.0
        ).astype(bf16)

    for g in range(steps):
        for c in group_copies[g]:
            c.wait()
        for s in range(g * GROUP, (g + 1) * GROUP):
            inside = dot(weights_s[s], values[s])
            heads = blocked[s]
            stacked = (
                heads[:, 0:KEY]
                + heads[:, KEY : 2 * KEY]
                + heads[:, 2 * KEY : 3 * KEY]
                + heads[:, 3 * KEY : 4 * KEY]
            )
            carried = jnp.concatenate(
                [dot(stacked, state[s, h].astype(bf16)) for h in range(HEADS)], axis=1
            )
            decay = jnp.exp((filled_of(s).astype(f32) + 1.0) * rate_tall)
            both = jnp.where(value_block, inside + carried * decay, 0.0)
            retained_s[s : s + 1, :] = jnp.sum(both, axis=0, keepdims=True)

    copies[8].wait()
    copies[9].wait()
    new_values = dot(normal_in, wv[...]).astype(bf16)
    new_values_o[...] = new_values
    new_values32 = new_values.astype(f32)
    headed = []
    for h in range(HEADS):
        own = jnp.sum(product[:, h * KEY : (h + 1) * KEY], axis=1, keepdims=True)
        own = own.astype(bf16).astype(f32)
        span = slice(h * VALUE, (h + 1) * VALUE)
        headed.append(normed(retained_s[:, span] + own * new_values32[:, span]).astype(bf16))
    copies[10].wait()
    mixer_out = dot(jnp.concatenate(headed, axis=1), wo[...])
    residual = widened + normed(mixer_out)
    residual_o[...] = residual
    normal_ffn = (normed(residual) * ffn_gain[...]).astype(bf16)
    ffn_o[...] = normal_ffn
    row = jnp.concatenate([normal_ffn, route_weight], axis=1)
    outgoing_o[...] = jnp.broadcast_to(row[None], outgoing_o.shape)
    for c in shard_copies:
        c.wait()


def mixer(
    tokens, lengths, mix_gain, ffn_gain, routes, scores, cache_keys, cache_values, state, wq, wk, wv, wo, gate, up, down
):
    shapes = [
        jax.ShapeDtypeStruct((SEQ, WIDTH), f32),
        jax.ShapeDtypeStruct((SEQ, WIDTH), bf16),
        jax.ShapeDtypeStruct((SEQ, HEADS * KEY), bf16),
        jax.ShapeDtypeStruct((SEQ, WIDTH), bf16),
        jax.ShapeDtypeStruct((NEAR, SEQ, WIDTH + EXPERTS), bf16),
        jax.ShapeDtypeStruct((3 * gate.shape[0], WIDTH), bf16),
    ]
    held = (
        routes.T, scores.T, tokens, mix_gain[None], wq, wk, cache_keys, wv, ffn_gain[None], wo, cache_values, state
    )
    return pl.pallas_call(
        mixer_kernel,
        name="mixer",
        out_shape=shapes,
        in_specs=[hbm] * 16,
        out_specs=[vmem] * 5 + [hbm],
        scratch_shapes=[pltpu.SMEM((SEQ,), jnp.int32)]
        + [pltpu.VMEM(a.shape, a.dtype) for a in held]
        + [
            pltpu.VMEM((SEQ, 8, BLOCK), bf16),
            pltpu.VMEM((SEQ, WIDTH), f32),
            pltpu.SemaphoreType.DMA((11,)),
            pltpu.SemaphoreType.DMA((2, SEQ // GROUP)),
            pltpu.SemaphoreType.DMA((3,)),
        ],
        cost_estimate=pl.CostEstimate(flops=2_000_000_000, bytes_accessed=22_000_000, transcendentals=0),
        compiler_params=pltpu.CompilerParams(vmem_limit_bytes=60 * MIB),
    )(lengths, *held, gate, up, down)


def swiglu(inputs, w_gate, w_up, w_down):
    hidden = (silu(dot(inputs, w_gate)) * dot(inputs, w_up)).astype(bf16)
    return dot(hidden, w_down)


def mixed(bits, masks):
    total = jnp.zeros_like(bits)
    for i, mask in enumerate(masks):
        total = total | (((bits >> i) & 1) * mask)
    return total


def select_kernel(index, near, outgoing_o, combine_o):
    tokens = near[:, :, 0:WIDTH].reshape(NEAR * SEQ, WIDTH)
    weights = near[:, :, WIDTH:].reshape(NEAR * SEQ, EXPERTS)
    expert = mixed(iota((EXPERTS, ROWS), 1) // HELD, far_masks) ^ index[0]
    pick = (iota((EXPERTS, ROWS), 0) == expert).astype(bf16)
    weight = dot(weights, pick)
    named = (weight > 0.0).astype(bf16)
    shape = (NEAR * SEQ, NEAR * SEQ)
    earlier = (iota(shape, 1) < iota(shape, 0)).astype(bf16)
    rank = dot(earlier, named)
    slot = (iota((NEAR * SEQ, ROWS), 1) % HELD).astype(f32)
    combine = jnp.where(rank == slot, weight, 0.0)
    combine_o[...] = combine.astype(bf16)
    chosen = dot_0((combine > 0.0).astype(bf16), tokens).astype(bf16)
    outgoing_o[...] = chosen.reshape(FAR, HELD, WIDTH)


def select(index, near):
    return pl.pallas_call(
        select_kernel,
        name="select",
        out_shape=[
            jax.ShapeDtypeStruct((FAR, HELD, WIDTH), bf16),
            jax.ShapeDtypeStruct((NEAR * SEQ, ROWS), bf16),
        ],
        in_specs=[pl.BlockSpec(memory_space=pltpu.SMEM), vmem],
        out_specs=[vmem] * 2,
        compiler_params=pltpu.CompilerParams(vmem_limit_bytes=8 * MIB),
    )(index, near)


def swiglu(inputs, w_gate, w_up, w_down):
    hidden = (silu(dot(inputs, w_gate)) * dot(inputs, w_up)).astype(bf16)
    return dot(hidden, w_down)


def expert_kernel(arrived, gate, up, down, back):
    rows = arrived[...].reshape(ROWS, WIDTH)
    out = swiglu(rows, gate[0], up[0], down[0]).astype(bf16)
    back[...] = out.reshape(FAR, HELD, WIDTH)


def experts(arrived, gate, up, down):
    return pl.pallas_call(
        expert_kernel,
        name="experts",
        out_shape=jax.ShapeDtypeStruct(arrived.shape, bf16),
        in_specs=[vmem] * 4,
        out_specs=vmem,
        cost_estimate=pl.CostEstimate(flops=500_000_000, bytes_accessed=3_000_000, transcendentals=0),
        compiler_params=pltpu.CompilerParams(vmem_limit_bytes=8 * MIB),
    )(arrived, gate, up, down)


def offsets(masks):
    found = [0]
    for m in masks:
        found = found + [f ^ m for f in found]
    return found


def dense_kernel(*refs):
    near, other, mix = refs[0:3]
    shards, own_o, other_o = refs[3:11], refs[11], refs[12]
    count = NEAR * SEQ
    inputs = jnp.concatenate(
        [t[:, :, 0:WIDTH].reshape(count, WIDTH) for t in (near, other)], axis=0
    )
    n = shards[0].shape[0] // 3
    gates, ups, downs = [
        jnp.concatenate([w[i * n : (i + 1) * n] for w in shards], axis=0) for i in range(3)
    ]
    hidden = (silu(dot_t(inputs, gates)) * dot_t(inputs, ups)).astype(bf16)
    part = (dot(hidden, downs) / (1.0 + jnp.exp(-mix[...]))).astype(bf16)
    own_o[...] = part[0:count].reshape(NEAR, SEQ, WIDTH)
    other_o[...] = part[count:].reshape(NEAR, SEQ, WIDTH)


def dense(near, other, weights, mix):
    part = jax.ShapeDtypeStruct((NEAR, SEQ, WIDTH), bf16)
    return pl.pallas_call(
        dense_kernel,
        name="dense",
        out_shape=[part] * 2,
        in_specs=[vmem] * 11,
        out_specs=[vmem] * 2,
        cost_estimate=pl.CostEstimate(flops=500_000_000, bytes_accessed=4_000_000, transcendentals=0),
        compiler_params=pltpu.CompilerParams(vmem_limit_bytes=12 * MIB),
    )(near, other, mix[None], *weights)


def combine_kernel(back, combine, own, other, parts_o):
    rows = back[...].reshape(ROWS, WIDTH)
    total = dot(combine[...], rows).reshape(NEAR, SEQ, WIDTH)
    parts_o[...] = (total + own[...].astype(f32) + other[...].astype(f32)).astype(bf16)


def combine_near(back, combine, own, other):
    return pl.pallas_call(
        combine_kernel,
        name="combine",
        out_shape=jax.ShapeDtypeStruct((NEAR, SEQ, WIDTH), bf16),
        in_specs=[vmem] * 4,
        out_specs=vmem,
        compiler_params=pltpu.CompilerParams(vmem_limit_bytes=8 * MIB),
    )(back, combine, own, other)


def shared_kernel(own, s_gate, s_up, s_down, out):
    out[...] = swiglu(own[...], s_gate[...], s_up[...], s_down[...])


def shared(own, s_gate, s_up, s_down):
    return pl.pallas_call(
        shared_kernel,
        name="shared",
        out_shape=jax.ShapeDtypeStruct((SEQ, WIDTH), f32),
        in_specs=[vmem] * 4,
        out_specs=vmem,
        cost_estimate=pl.CostEstimate(flops=900_000_000, bytes_accessed=2_000_000, transcendentals=0),
        compiler_params=pltpu.CompilerParams(vmem_limit_bytes=4 * MIB),
    )(own, s_gate, s_up, s_down)


def final_kernel(parts, residual, extra, out):
    combined = extra[...] + jnp.sum(parts[...].astype(f32), axis=0)
    out[...] = (residual[...] + normed(combined)).astype(bf16)


def final(parts, residual, extra):
    return pl.pallas_call(
        final_kernel,
        name="final",
        out_shape=jax.ShapeDtypeStruct(residual.shape, bf16),
        in_specs=[vmem] * 3,
        out_specs=vmem,
        compiler_params=pltpu.CompilerParams(vmem_limit_bytes=4 * MIB),
    )(parts, residual, extra)


near_groups = [[r ^ f for r in offsets(near_masks)] for f in offsets(far_masks)]
far_groups = [[r ^ f for f in offsets(far_masks)] for r in offsets(near_masks)]


def exchange(values, groups):
    return lax.all_to_all(
        values, "ep", split_axis=0, concat_axis=0, axis_index_groups=groups, tiled=True
    )


def per_device(
    tokens,
    lengths,
    cache_keys,
    cache_values,
    retention_state,
    mix_gain,
    query_weight,
    key_weight,
    value_weight,
    out_weight,
    ffn_gain,
    routes,
    route_scores,
    expert_gate,
    expert_up,
    expert_down,
    shared_gate,
    shared_up,
    shared_down,
    dense_gate,
    dense_up,
    dense_down,
    dense_mix,
):
    residual, normal_ffn, new_keys, new_values, outgoing, shard = mixer(
        tokens,
        lengths,
        mix_gain,
        ffn_gain,
        routes,
        route_scores,
        cache_keys,
        cache_values,
        retention_state,
        query_weight,
        key_weight,
        value_weight,
        out_weight,
        dense_gate,
        dense_up,
        dense_down,
    )
    hop = {}
    for m in (2, 8, 32):
        hop[m] = flip(shard, m)
    for m, k in ((2, 8), (8, 32), (32, 2)):
        hop[m | k] = flip(hop[m], k)
    hop[42] = flip(hop[10], 32)
    weights = [shard] + list(hop.values())

    near = exchange(outgoing, near_groups)
    place = lax.axis_index("ep").astype(jnp.int32)
    index = mixed((place >> 2) & 1 | (place >> 3) & 2 | (place >> 4) & 4, near_masks)
    chosen, combine = select(index[None], near)
    other = flip(near, 1)
    own_part, other_part = dense(near, other, weights, dense_mix)
    arrived = exchange(chosen, far_groups)
    outputs = experts(arrived, expert_gate, expert_up, expert_down)
    back = exchange(outputs, far_groups)
    other_part = flip(other_part, 1)
    parts = combine_near(back, combine, own_part, other_part)
    parts = exchange(parts, near_groups)
    extra = shared(normal_ffn, shared_gate, shared_up, shared_down)
    layer_out = final(parts, residual, extra)
    return (layer_out, new_keys, new_values)


def solution(mesh):
    in_specs = (
        P("ep", None),
        P("ep"),
        P("ep", None, None),
        P("ep", None, None),
        P("ep", None, None, None),
        P(),
        P(),
        P(),
        P(),
        P(),
        P(),
        P("ep", None),
        P("ep", None),
        P("ep", None, None),
        P("ep", None, None),
        P("ep", None, None),
        P(),
        P(),
        P(),
        P("ep", None),
        P("ep", None),
        P("ep", None),
        P(),
    )
    out_specs = (P("ep", None), P("ep", None), P("ep", None))

    return jax.shard_map(
        per_device, mesh=mesh, in_specs=in_specs, out_specs=out_specs, check_vma=False
    )
```

```python
import math

import jax
import jax.numpy as jnp
from jax import lax
from jax.experimental import pallas as pl
from jax.experimental.pallas import tpu as pltpu
from jax.sharding import PartitionSpec as P


eps = 1e-06
route_scale = 2.5
rope_base = 10000.0

SEQ = 16
WIDTH = 1024
HEADS = 4
KEY = 128
VALUE = 256
BLOCK = 128
EXPERTS = 128
SLOTS = 2
NEAR = 8
FAR = 16
HELD = SLOTS * NEAR
ROWS = FAR * HELD
GROUP = 4
MIB = 1024 * 1024

near_masks = (1, 2, 4)
far_masks = (8, 16, 32, 64)
wide_mask = 8
weight_masks = (32, 96, 24)

f32 = jnp.float32
bf16 = jnp.bfloat16
vmem = pl.BlockSpec(memory_space=pltpu.VMEM)
hbm = pl.BlockSpec(memory_space=pltpu.HBM)


def flip(values, mask):
    return lax.ppermute(values, "ep", [(i, i ^ mask) for i in range(lax.axis_size("ep"))])


def normed(values):
    return values * lax.rsqrt(jnp.mean(values * values, axis=-1, keepdims=True) + eps)


def dot(a, b):
    return jnp.dot(a, b, preferred_element_type=f32)


def dot_t(a, b):
    return lax.dot_general(a, b, (((1,), (1,)), ((), ())), preferred_element_type=f32)


def dot_0(a, b):
    return lax.dot_general(a, b, (((0,), (0,)), ((), ())), preferred_element_type=f32)


def iota(shape, axis):
    return lax.broadcasted_iota(jnp.int32, shape, axis)


def silu(v):
    return v / (1.0 + jnp.exp(-v))


def head_rates(head_ids):
    return jnp.log1p(-jnp.exp2(-5.0 - head_ids.astype(f32)))


def rotary(length_of):
    shape = (SEQ, KEY)
    row = iota(shape, 0)
    half = KEY // 2
    position = jnp.zeros(shape, f32)
    for s in range(SEQ):
        position = jnp.where(row == s, length_of(s).astype(f32), position)
    lane = iota(shape, 1)
    inverse = jnp.exp((lane % half).astype(f32) * (-math.log(rope_base) / half))
    angles = position * inverse
    sine = jnp.sin(angles)
    return jnp.cos(angles), jnp.where(lane < half, -sine, sine)


def route_weights(routes, scores):
    expert = iota((EXPERTS, SEQ), 0)
    weight = scores / jnp.sum(scores, axis=0, keepdims=True) * route_scale
    weighted = jnp.zeros((EXPERTS, SEQ), f32)
    for k in range(routes.shape[0]):
        weighted = jnp.where(routes[k : k + 1, :] == expert, weight[k : k + 1, :], weighted)
    same = (iota((EXPERTS, EXPERTS), 0) == iota((EXPERTS, EXPERTS), 1)).astype(bf16)
    return dot_0(weighted.astype(bf16), same).astype(bf16)


def mixer_kernel(
    lengths_h,
    routes_h,
    scores_h,
    tokens_h,
    mix_gain_h,
    wq_h,
    wk_h,
    keys_h,
    wv_h,
    ffn_gain_h,
    wo_h,
    values_h,
    state_h,
    gate_h,
    up_h,
    down_h,
    residual_o,
    ffn_o,
    new_keys_o,
    new_values_o,
    outgoing_o,
    shard_o,
    lengths_s,
    routes_s,
    scores_s,
    tokens_s,
    mix_gain,
    wq,
    wk,
    keys,
    wv,
    ffn_gain,
    wo,
    values,
    state,
    weights_s,
    retained_s,
    sems,
    group_sems,
    shard_sems,
):
    sources = (
        lengths_h, routes_h, scores_h, tokens_h, mix_gain_h, wq_h, wk_h, keys_h, wv_h, ffn_gain_h, wo_h
    )
    targets = (
        lengths_s, routes_s, scores_s, tokens_s, mix_gain, wq, wk, keys, wv, ffn_gain, wo
    )
    copies = [
        pltpu.make_async_copy(src, dst, sems.at[i])
        for i, (src, dst) in enumerate(zip(sources, targets))
    ]
    steps = SEQ // GROUP
    group_copies = []
    for g in range(steps):
        part = pl.ds(g * GROUP, GROUP)
        group_copies.append(
            (
                pltpu.make_async_copy(values_h.at[part], values.at[part], group_sems.at[0, g]),
                pltpu.make_async_copy(state_h.at[part], state.at[part], group_sems.at[1, g]),
            )
        )
    for c in copies[:8]:
        c.start()
    for c in group_copies[0]:
        c.start()
    for c in copies[8:10]:
        c.start()
    for pair in group_copies[1:]:
        for c in pair:
            c.start()
    copies[10].start()
    rows = gate_h.shape[0]
    shard_copies = [
        pltpu.make_async_copy(src, shard_o.at[pl.ds(i * rows, rows)], shard_sems.at[i])
        for i, src in enumerate((gate_h, up_h, down_h))
    ]
    for c in shard_copies:
        c.start()
    for c in copies[:3]:
        c.wait()

    def filled_of(s):
        return lax.rem(lengths_s[s], BLOCK)

    route_weight = route_weights(routes_s[...], scores_s[...])

    cosine, sine = rotary(lambda s: lengths_s[s])
    cos = jnp.concatenate([cosine] * HEADS, axis=1)
    sin = jnp.concatenate([sine] * HEADS, axis=1)
    copies[3].wait()
    copies[4].wait()
    widened = tokens_s[...].astype(f32)
    normal_in = (normed(widened) * mix_gain[...]).astype(bf16)

    def rotate(raw):
        swapped = jnp.concatenate(
            [pltpu.roll(raw[:, h * KEY : (h + 1) * KEY], KEY // 2, 1) for h in range(HEADS)],
            axis=1,
        )
        return raw * cos + swapped * sin

    copies[5].wait()
    copies[6].wait()
    queries = (rotate(dot(normal_in, wq[...])) * KEY ** (-0.5)).astype(bf16)
    new_keys = rotate(dot(normal_in, wk[...])).astype(bf16)
    new_keys_o[...] = new_keys
    queries32 = queries.astype(f32)
    product = queries32 * new_keys.astype(f32)

    head_of = iota((8, HEADS * KEY), 0)
    query_block = iota((8, HEADS * KEY), 1) // KEY == head_of
    place = iota((8, BLOCK), 1)
    rate_wide = head_rates(iota((8, BLOCK), 0))
    rate_tall = head_rates(iota((8, 1), 0))
    value_block = iota((8, HEADS * VALUE), 1) // VALUE == iota((8, HEADS * VALUE), 0)

    blocked = []
    copies[7].wait()
    for s in range(SEQ):
        spread_query = jnp.where(
            query_block, jnp.broadcast_to(queries32[s : s + 1], (8, HEADS * KEY)), 0.0
        ).astype(bf16)
        blocked.append(spread_query)
        found = dot_t(spread_query, keys[s])
        distance = jnp.maximum(filled_of(s) - place, 0).astype(f32)
        weights_s[s] = jnp.where(
            place < filled_of(s), found * jnp.exp(distance * rate_wide), 0.0
        ).astype(bf16)

    for g in range(steps):
        for c in group_copies[g]:
            c.wait()
        for s in range(g * GROUP, (g + 1) * GROUP):
            inside = dot(weights_s[s], values[s])
            heads = blocked[s]
            stacked = (
                heads[:, 0:KEY]
                + heads[:, KEY : 2 * KEY]
                + heads[:, 2 * KEY : 3 * KEY]
                + heads[:, 3 * KEY : 4 * KEY]
            )
            carried = jnp.concatenate(
                [dot(stacked, state[s, h].astype(bf16)) for h in range(HEADS)], axis=1
            )
            decay = jnp.exp((filled_of(s).astype(f32) + 1.0) * rate_tall)
            both = jnp.where(value_block, inside + carried * decay, 0.0)
            retained_s[s : s + 1, :] = jnp.sum(both, axis=0, keepdims=True)

    copies[8].wait()
    copies[9].wait()
    new_values = dot(normal_in, wv[...]).astype(bf16)
    new_values_o[...] = new_values
    new_values32 = new_values.astype(f32)
    headed = []
    for h in range(HEADS):
        own = jnp.sum(product[:, h * KEY : (h + 1) * KEY], axis=1, keepdims=True)
        own = own.astype(bf16).astype(f32)
        span = slice(h * VALUE, (h + 1) * VALUE)
        headed.append(normed(retained_s[:, span] + own * new_values32[:, span]).astype(bf16))
    copies[10].wait()
    mixer_out = dot(jnp.concatenate(headed, axis=1), wo[...])
    residual = widened + normed(mixer_out)
    residual_o[...] = residual
    normal_ffn = (normed(residual) * ffn_gain[...]).astype(bf16)
    ffn_o[...] = normal_ffn
    row = jnp.concatenate([normal_ffn, route_weight], axis=1)
    outgoing_o[...] = jnp.broadcast_to(row[None], outgoing_o.shape)
    for c in shard_copies:
        c.wait()


def mixer(
    tokens, lengths, mix_gain, ffn_gain, routes, scores, cache_keys, cache_values, state, wq, wk, wv, wo, gate, up, down
):
    shapes = [
        jax.ShapeDtypeStruct((SEQ, WIDTH), f32),
        jax.ShapeDtypeStruct((SEQ, WIDTH), bf16),
        jax.ShapeDtypeStruct((SEQ, HEADS * KEY), bf16),
        jax.ShapeDtypeStruct((SEQ, WIDTH), bf16),
        jax.ShapeDtypeStruct((NEAR, SEQ, WIDTH + EXPERTS), bf16),
        jax.ShapeDtypeStruct((3 * gate.shape[0], WIDTH), bf16),
    ]
    held = (
        routes.T, scores.T, tokens, mix_gain[None], wq, wk, cache_keys, wv, ffn_gain[None], wo, cache_values, state
    )
    return pl.pallas_call(
        mixer_kernel,
        name="mixer",
        out_shape=shapes,
        in_specs=[hbm] * 16,
        out_specs=[vmem] * 5 + [hbm],
        scratch_shapes=[pltpu.SMEM((SEQ,), jnp.int32)]
        + [pltpu.VMEM(a.shape, a.dtype) for a in held]
        + [
            pltpu.VMEM((SEQ, 8, BLOCK), bf16),
            pltpu.VMEM((SEQ, WIDTH), f32),
            pltpu.SemaphoreType.DMA((11,)),
            pltpu.SemaphoreType.DMA((2, SEQ // GROUP)),
            pltpu.SemaphoreType.DMA((3,)),
        ],
        cost_estimate=pl.CostEstimate(flops=2_000_000_000, bytes_accessed=22_000_000, transcendentals=0),
        compiler_params=pltpu.CompilerParams(vmem_limit_bytes=60 * MIB),
    )(lengths, *held, gate, up, down)


def swiglu(inputs, w_gate, w_up, w_down):
    hidden = (silu(dot(inputs, w_gate)) * dot(inputs, w_up)).astype(bf16)
    return dot(hidden, w_down)


def mixed(bits, masks):
    total = jnp.zeros_like(bits)
    for i, mask in enumerate(masks):
        total = total | (((bits >> i) & 1) * mask)
    return total


def select_kernel(index, near, outgoing_o, combine_o):
    tokens = near[:, :, 0:WIDTH].reshape(NEAR * SEQ, WIDTH)
    weights = near[:, :, WIDTH:].reshape(NEAR * SEQ, EXPERTS)
    expert = mixed(iota((EXPERTS, ROWS), 1) // HELD, far_masks) ^ index[0]
    pick = (iota((EXPERTS, ROWS), 0) == expert).astype(bf16)
    weight = dot(weights, pick)
    named = (weight > 0.0).astype(bf16)
    shape = (NEAR * SEQ, NEAR * SEQ)
    earlier = (iota(shape, 1) < iota(shape, 0)).astype(bf16)
    rank = dot(earlier, named)
    slot = (iota((NEAR * SEQ, ROWS), 1) % HELD).astype(f32)
    combine = jnp.where(rank == slot, weight, 0.0)
    combine_o[...] = combine.astype(bf16)
    chosen = dot_0((combine > 0.0).astype(bf16), tokens).astype(bf16)
    outgoing_o[...] = chosen.reshape(FAR, HELD, WIDTH)


def select(index, near):
    return pl.pallas_call(
        select_kernel,
        name="select",
        out_shape=[
            jax.ShapeDtypeStruct((FAR, HELD, WIDTH), bf16),
            jax.ShapeDtypeStruct((NEAR * SEQ, ROWS), bf16),
        ],
        in_specs=[pl.BlockSpec(memory_space=pltpu.SMEM), vmem],
        out_specs=[vmem] * 2,
        compiler_params=pltpu.CompilerParams(vmem_limit_bytes=8 * MIB),
    )(index, near)


def swiglu(inputs, w_gate, w_up, w_down):
    hidden = (silu(dot(inputs, w_gate)) * dot(inputs, w_up)).astype(bf16)
    return dot(hidden, w_down)


def expert_kernel(arrived, gate, up, down, back):
    rows = arrived[...].reshape(ROWS, WIDTH)
    out = swiglu(rows, gate[0], up[0], down[0]).astype(bf16)
    back[...] = out.reshape(FAR, HELD, WIDTH)


def experts(arrived, gate, up, down):
    return pl.pallas_call(
        expert_kernel,
        name="experts",
        out_shape=jax.ShapeDtypeStruct(arrived.shape, bf16),
        in_specs=[vmem] * 4,
        out_specs=vmem,
        cost_estimate=pl.CostEstimate(flops=500_000_000, bytes_accessed=3_000_000, transcendentals=0),
        compiler_params=pltpu.CompilerParams(vmem_limit_bytes=8 * MIB),
    )(arrived, gate, up, down)


def offsets(masks):
    found = [0]
    for m in masks:
        found = found + [f ^ m for f in found]
    return found


def dense_kernel(*refs):
    near, other, mix = refs[0:3]
    shards, own_o, other_o = refs[3:11], refs[11], refs[12]
    count = NEAR * SEQ
    inputs = jnp.concatenate(
        [t[:, :, 0:WIDTH].reshape(count, WIDTH) for t in (near, other)], axis=0
    )
    n = shards[0].shape[0] // 3
    gates, ups, downs = [
        jnp.concatenate([w[i * n : (i + 1) * n] for w in shards], axis=0) for i in range(3)
    ]
    hidden = (silu(dot_t(inputs, gates)) * dot_t(inputs, ups)).astype(bf16)
    part = (dot(hidden, downs) / (1.0 + jnp.exp(-mix[...]))).astype(bf16)
    own_o[...] = part[0:count].reshape(NEAR, SEQ, WIDTH)
    other_o[...] = part[count:].reshape(NEAR, SEQ, WIDTH)


def dense(near, other, weights, mix):
    part = jax.ShapeDtypeStruct((NEAR, SEQ, WIDTH), bf16)
    return pl.pallas_call(
        dense_kernel,
        name="dense",
        out_shape=[part] * 2,
        in_specs=[vmem] * 11,
        out_specs=[vmem] * 2,
        cost_estimate=pl.CostEstimate(flops=500_000_000, bytes_accessed=4_000_000, transcendentals=0),
        compiler_params=pltpu.CompilerParams(vmem_limit_bytes=12 * MIB),
    )(near, other, mix[None], *weights)


def combine_kernel(place, back, combine, own, other, keep_o, send_o, total_s):
    rows = back[...].reshape(ROWS, WIDTH)
    total = dot(combine[...], rows).reshape(NEAR, SEQ, WIDTH)
    total_s[...] = total + own[...].astype(f32) + other[...].astype(f32)
    for j, k in enumerate((0, 6, 2, 4)):
        span = slice(j * SEQ, (j + 1) * SEQ)
        keep_o[span] = total_s[place[0] ^ k]
        send_o[span] = total_s[place[0] ^ (k + 1)].astype(bf16)


def halves(rows):
    return [
        jax.ShapeDtypeStruct((rows // 2, WIDTH), f32),
        jax.ShapeDtypeStruct((rows // 2, WIDTH), bf16),
    ]


def combine_near(place, back, combine, own, other):
    return pl.pallas_call(
        combine_kernel,
        name="combine",
        out_shape=halves(NEAR * SEQ),
        in_specs=[pl.BlockSpec(memory_space=pltpu.SMEM)] + [vmem] * 4,
        out_specs=[vmem] * 2,
        scratch_shapes=[pltpu.VMEM((NEAR, SEQ, WIDTH), f32)],
        compiler_params=pltpu.CompilerParams(vmem_limit_bytes=8 * MIB),
    )(place, back, combine, own, other)


def fold_kernel(kept, came, keep_o, send_o):
    total = kept[...] + came[...].astype(f32)
    half = total.shape[0] // 2
    keep_o[...] = total[0:half]
    send_o[...] = total[half:].astype(bf16)


def fold(kept, came):
    return pl.pallas_call(
        fold_kernel,
        name="fold",
        out_shape=halves(kept.shape[0]),
        in_specs=[vmem] * 2,
        out_specs=[vmem] * 2,
        compiler_params=pltpu.CompilerParams(vmem_limit_bytes=2 * MIB),
    )(kept, came)


def shared_kernel(own, s_gate, s_up, s_down, out):
    out[...] = swiglu(own[...], s_gate[...], s_up[...], s_down[...])


def shared(own, s_gate, s_up, s_down):
    return pl.pallas_call(
        shared_kernel,
        name="shared",
        out_shape=jax.ShapeDtypeStruct((SEQ, WIDTH), f32),
        in_specs=[vmem] * 4,
        out_specs=vmem,
        cost_estimate=pl.CostEstimate(flops=900_000_000, bytes_accessed=2_000_000, transcendentals=0),
        compiler_params=pltpu.CompilerParams(vmem_limit_bytes=4 * MIB),
    )(own, s_gate, s_up, s_down)


def final_kernel(kept, came, residual, extra, out):
    combined = extra[...] + kept[...] + came[...].astype(f32)
    out[...] = (residual[...] + normed(combined)).astype(bf16)


def final(kept, came, residual, extra):
    return pl.pallas_call(
        final_kernel,
        name="final",
        out_shape=jax.ShapeDtypeStruct(residual.shape, bf16),
        in_specs=[vmem] * 4,
        out_specs=vmem,
        compiler_params=pltpu.CompilerParams(vmem_limit_bytes=4 * MIB),
    )(kept, came, residual, extra)


near_groups = [[r ^ f for r in offsets(near_masks)] for f in offsets(far_masks)]
far_groups = [[r ^ f for f in offsets(far_masks)] for r in offsets(near_masks)]


def exchange(values, groups):
    return lax.all_to_all(
        values, "ep", split_axis=0, concat_axis=0, axis_index_groups=groups, tiled=True
    )


def per_device(
    tokens,
    lengths,
    cache_keys,
    cache_values,
    retention_state,
    mix_gain,
    query_weight,
    key_weight,
    value_weight,
    out_weight,
    ffn_gain,
    routes,
    route_scores,
    expert_gate,
    expert_up,
    expert_down,
    shared_gate,
    shared_up,
    shared_down,
    dense_gate,
    dense_up,
    dense_down,
    dense_mix,
):
    residual, normal_ffn, new_keys, new_values, outgoing, shard = mixer(
        tokens,
        lengths,
        mix_gain,
        ffn_gain,
        routes,
        route_scores,
        cache_keys,
        cache_values,
        retention_state,
        query_weight,
        key_weight,
        value_weight,
        out_weight,
        dense_gate,
        dense_up,
        dense_down,
    )
    hop = {}
    for m in weight_masks:
        hop[m] = flip(shard, m)
    first, second, third = weight_masks
    for m, k in ((first, second), (second, third), (third, first)):
        hop[m ^ k] = flip(hop[m], k)
    hop[first ^ second ^ third] = flip(hop[first ^ second], third)
    weights = [shard] + list(hop.values())

    near = exchange(outgoing, near_groups)
    place = lax.axis_index("ep").astype(jnp.int32)
    index = place & 7
    chosen, combine = select(index[None], near)
    other = flip(near, wide_mask)
    own_part, other_part = dense(near, other, weights, dense_mix)
    arrived = exchange(chosen, far_groups)
    outputs = experts(arrived, expert_gate, expert_up, expert_down)
    back = exchange(outputs, far_groups)
    other_part = flip(other_part, wide_mask)
    kept, sent = combine_near(index[None], back, combine, own_part, other_part)
    for m in (1, 2):
        came = flip(sent, m)
        kept, sent = fold(kept, came)
    came = flip(sent, 6)
    extra = shared(normal_ffn, shared_gate, shared_up, shared_down)
    layer_out = final(kept, came, residual, extra)
    return (layer_out, new_keys, new_values)


def solution(mesh):
    in_specs = (
        P("ep", None),
        P("ep"),
        P("ep", None, None),
        P("ep", None, None),
        P("ep", None, None, None),
        P(),
        P(),
        P(),
        P(),
        P(),
        P(),
        P("ep", None),
        P("ep", None),
        P("ep", None, None),
        P("ep", None, None),
        P("ep", None, None),
        P(),
        P(),
        P(),
        P("ep", None),
        P("ep", None),
        P("ep", None),
        P(),
    )
    out_specs = (P("ep", None), P("ep", None), P("ep", None))

    return jax.shard_map(
        per_device, mesh=mesh, in_specs=in_specs, out_specs=out_specs, check_vma=False
    )
```

```python
import math

import jax
import jax.numpy as jnp
from jax import lax
from jax.experimental import pallas as pl
from jax.experimental.pallas import tpu as pltpu
from jax.sharding import PartitionSpec as P


eps = 1e-06
route_scale = 2.5
rope_base = 10000.0

SEQ = 16
WIDTH = 1024
HEADS = 4
KEY = 128
VALUE = 256
BLOCK = 128
EXPERTS = 128
SLOTS = 2
NEAR = 8
FAR = 16
HELD = SLOTS * NEAR
ROWS = FAR * HELD
GROUP = 4
MIB = 1024 * 1024

near_masks = (1, 2, 4)
far_masks = (8, 16, 32, 64)
wide_mask = 8
weight_masks = (32, 96, 24)

f32 = jnp.float32
bf16 = jnp.bfloat16
vmem = pl.BlockSpec(memory_space=pltpu.VMEM)
hbm = pl.BlockSpec(memory_space=pltpu.HBM)


def flip(values, mask):
    return lax.ppermute(values, "ep", [(i, i ^ mask) for i in range(lax.axis_size("ep"))])


def normed(values):
    return values * lax.rsqrt(jnp.mean(values * values, axis=-1, keepdims=True) + eps)


def dot(a, b):
    return jnp.dot(a, b, preferred_element_type=f32)


def dot_t(a, b):
    return lax.dot_general(a, b, (((1,), (1,)), ((), ())), preferred_element_type=f32)


def dot_0(a, b):
    return lax.dot_general(a, b, (((0,), (0,)), ((), ())), preferred_element_type=f32)


def iota(shape, axis):
    return lax.broadcasted_iota(jnp.int32, shape, axis)


def silu(v):
    return v / (1.0 + jnp.exp(-v))


def head_rates(head_ids):
    return jnp.log1p(-jnp.exp2(-5.0 - head_ids.astype(f32)))


def rotary(length_of):
    shape = (SEQ, KEY)
    row = iota(shape, 0)
    half = KEY // 2
    position = jnp.zeros(shape, f32)
    for s in range(SEQ):
        position = jnp.where(row == s, length_of(s).astype(f32), position)
    lane = iota(shape, 1)
    inverse = jnp.exp((lane % half).astype(f32) * (-math.log(rope_base) / half))
    angles = position * inverse
    sine = jnp.sin(angles)
    return jnp.cos(angles), jnp.where(lane < half, -sine, sine)


def route_weights(routes, scores):
    expert = iota((EXPERTS, SEQ), 0)
    weight = scores / jnp.sum(scores, axis=0, keepdims=True) * route_scale
    weighted = jnp.zeros((EXPERTS, SEQ), f32)
    for k in range(routes.shape[0]):
        weighted = jnp.where(routes[k : k + 1, :] == expert, weight[k : k + 1, :], weighted)
    same = (iota((EXPERTS, EXPERTS), 0) == iota((EXPERTS, EXPERTS), 1)).astype(bf16)
    return dot_0(weighted.astype(bf16), same).astype(bf16)


def mixer_kernel(
    lengths_h,
    routes_h,
    scores_h,
    tokens_h,
    mix_gain_h,
    wq_h,
    wk_h,
    keys_h,
    wv_h,
    ffn_gain_h,
    wo_h,
    values_h,
    state_h,
    gate_h,
    up_h,
    down_h,
    residual_o,
    ffn_o,
    new_keys_o,
    new_values_o,
    outgoing_o,
    shard_o,
    lengths_s,
    routes_s,
    scores_s,
    tokens_s,
    mix_gain,
    wq,
    wk,
    keys,
    wv,
    ffn_gain,
    wo,
    values,
    state,
    weights_s,
    retained_s,
    sems,
    group_sems,
    shard_sems,
):
    sources = (
        lengths_h, routes_h, scores_h, tokens_h, mix_gain_h, wq_h, wk_h, keys_h, wv_h, ffn_gain_h, wo_h
    )
    targets = (
        lengths_s, routes_s, scores_s, tokens_s, mix_gain, wq, wk, keys, wv, ffn_gain, wo
    )
    copies = [
        pltpu.make_async_copy(src, dst, sems.at[i])
        for i, (src, dst) in enumerate(zip(sources, targets))
    ]
    steps = SEQ // GROUP
    group_copies = []
    for g in range(steps):
        part = pl.ds(g * GROUP, GROUP)
        group_copies.append(
            (
                pltpu.make_async_copy(values_h.at[part], values.at[part], group_sems.at[0, g]),
                pltpu.make_async_copy(state_h.at[part], state.at[part], group_sems.at[1, g]),
            )
        )
    for c in copies[:8]:
        c.start()
    for c in group_copies[0]:
        c.start()
    for c in copies[8:10]:
        c.start()
    for pair in group_copies[1:]:
        for c in pair:
            c.start()
    copies[10].start()
    rows = gate_h.shape[0]
    shard_copies = [
        pltpu.make_async_copy(src, shard_o.at[pl.ds(i * rows, rows)], shard_sems.at[i])
        for i, src in enumerate((gate_h, up_h, down_h))
    ]
    for c in shard_copies:
        c.start()
    for c in copies[:3]:
        c.wait()

    def filled_of(s):
        return lax.rem(lengths_s[s], BLOCK)

    route_weight = route_weights(routes_s[...], scores_s[...])

    cosine, sine = rotary(lambda s: lengths_s[s])
    cos = jnp.concatenate([cosine] * HEADS, axis=1)
    sin = jnp.concatenate([sine] * HEADS, axis=1)
    copies[3].wait()
    copies[4].wait()
    widened = tokens_s[...].astype(f32)
    normal_in = (normed(widened) * mix_gain[...]).astype(bf16)

    def rotate(raw):
        swapped = jnp.concatenate(
            [pltpu.roll(raw[:, h * KEY : (h + 1) * KEY], KEY // 2, 1) for h in range(HEADS)],
            axis=1,
        )
        return raw * cos + swapped * sin

    copies[5].wait()
    copies[6].wait()
    queries = (rotate(dot(normal_in, wq[...])) * KEY ** (-0.5)).astype(bf16)
    new_keys = rotate(dot(normal_in, wk[...])).astype(bf16)
    new_keys_o[...] = new_keys
    queries32 = queries.astype(f32)
    product = queries32 * new_keys.astype(f32)

    head_of = iota((8, HEADS * KEY), 0)
    query_block = iota((8, HEADS * KEY), 1) // KEY == head_of
    place = iota((8, BLOCK), 1)
    rate_wide = head_rates(iota((8, BLOCK), 0))
    rate_tall = head_rates(iota((8, 1), 0))
    value_block = iota((8, HEADS * VALUE), 1) // VALUE == iota((8, HEADS * VALUE), 0)

    blocked = []
    copies[7].wait()
    for s in range(SEQ):
        spread_query = jnp.where(
            query_block, jnp.broadcast_to(queries32[s : s + 1], (8, HEADS * KEY)), 0.0
        ).astype(bf16)
        blocked.append(spread_query)
        found = dot_t(spread_query, keys[s])
        distance = jnp.maximum(filled_of(s) - place, 0).astype(f32)
        weights_s[s] = jnp.where(
            place < filled_of(s), found * jnp.exp(distance * rate_wide), 0.0
        ).astype(bf16)

    def settle(found):
        for s, inside, carried in found:
            decay = jnp.exp((filled_of(s).astype(f32) + 1.0) * rate_tall)
            both = jnp.where(value_block, inside + carried * decay, 0.0)
            retained_s[s : s + 1, :] = jnp.sum(both, axis=0, keepdims=True)

    pending = []
    for g in range(steps):
        for c in group_copies[g]:
            c.wait()
        found = []
        for s in range(g * GROUP, (g + 1) * GROUP):
            inside = dot(weights_s[s], values[s])
            heads = blocked[s]
            stacked = (
                heads[:, 0:KEY]
                + heads[:, KEY : 2 * KEY]
                + heads[:, 2 * KEY : 3 * KEY]
                + heads[:, 3 * KEY : 4 * KEY]
            )
            carried = jnp.concatenate(
                [dot(stacked, state[s, h].astype(bf16)) for h in range(HEADS)], axis=1
            )
            found.append((s, inside, carried))
        settle(pending)
        pending = found
        if g == 1:
            copies[8].wait()
            new_values = dot(normal_in, wv[...]).astype(bf16)
            new_values_o[...] = new_values
    settle(pending)

    copies[9].wait()
    new_values32 = new_values.astype(f32)
    headed = []
    for h in range(HEADS):
        own = jnp.sum(product[:, h * KEY : (h + 1) * KEY], axis=1, keepdims=True)
        own = own.astype(bf16).astype(f32)
        span = slice(h * VALUE, (h + 1) * VALUE)
        headed.append(normed(retained_s[:, span] + own * new_values32[:, span]).astype(bf16))
    copies[10].wait()
    mixer_out = dot(jnp.concatenate(headed, axis=1), wo[...])
    residual = widened + normed(mixer_out)
    residual_o[...] = residual
    normal_ffn = (normed(residual) * ffn_gain[...]).astype(bf16)
    ffn_o[...] = normal_ffn
    row = jnp.concatenate([normal_ffn, route_weight], axis=1)
    outgoing_o[...] = jnp.broadcast_to(row[None], outgoing_o.shape)
    for c in shard_copies:
        c.wait()


def mixer(
    tokens, lengths, mix_gain, ffn_gain, routes, scores, cache_keys, cache_values, state, wq, wk, wv, wo, gate, up, down
):
    shapes = [
        jax.ShapeDtypeStruct((SEQ, WIDTH), f32),
        jax.ShapeDtypeStruct((SEQ, WIDTH), bf16),
        jax.ShapeDtypeStruct((SEQ, HEADS * KEY), bf16),
        jax.ShapeDtypeStruct((SEQ, WIDTH), bf16),
        jax.ShapeDtypeStruct((NEAR, SEQ, WIDTH + EXPERTS), bf16),
        jax.ShapeDtypeStruct((3 * gate.shape[0], WIDTH), bf16),
    ]
    held = (
        routes.T, scores.T, tokens, mix_gain[None], wq, wk, cache_keys, wv, ffn_gain[None], wo, cache_values, state
    )
    return pl.pallas_call(
        mixer_kernel,
        name="mixer",
        out_shape=shapes,
        in_specs=[hbm] * 16,
        out_specs=[vmem] * 5 + [hbm],
        scratch_shapes=[pltpu.SMEM((SEQ,), jnp.int32)]
        + [pltpu.VMEM(a.shape, a.dtype) for a in held]
        + [
            pltpu.VMEM((SEQ, 8, BLOCK), bf16),
            pltpu.VMEM((SEQ, WIDTH), f32),
            pltpu.SemaphoreType.DMA((11,)),
            pltpu.SemaphoreType.DMA((2, SEQ // GROUP)),
            pltpu.SemaphoreType.DMA((3,)),
        ],
        cost_estimate=pl.CostEstimate(flops=2_000_000_000, bytes_accessed=22_000_000, transcendentals=0),
        compiler_params=pltpu.CompilerParams(vmem_limit_bytes=60 * MIB),
    )(lengths, *held, gate, up, down)


def swiglu(inputs, w_gate, w_up, w_down):
    hidden = (silu(dot(inputs, w_gate)) * dot(inputs, w_up)).astype(bf16)
    return dot(hidden, w_down)


def mixed(bits, masks):
    total = jnp.zeros_like(bits)
    for i, mask in enumerate(masks):
        total = total | (((bits >> i) & 1) * mask)
    return total


def select_kernel(index, near, outgoing_o, combine_o):
    tokens = near[:, :, 0:WIDTH].reshape(NEAR * SEQ, WIDTH)
    weights = near[:, :, WIDTH:].reshape(NEAR * SEQ, EXPERTS)
    expert = mixed(iota((EXPERTS, ROWS), 1) // HELD, far_masks) ^ index[0]
    pick = (iota((EXPERTS, ROWS), 0) == expert).astype(bf16)
    weight = dot(weights, pick)
    named = (weight > 0.0).astype(bf16)
    shape = (NEAR * SEQ, NEAR * SEQ)
    earlier = (iota(shape, 1) < iota(shape, 0)).astype(bf16)
    rank = dot(earlier, named)
    slot = (iota((NEAR * SEQ, ROWS), 1) % HELD).astype(f32)
    combine = jnp.where(rank == slot, weight, 0.0)
    combine_o[...] = combine.astype(bf16)
    chosen = dot_0((combine > 0.0).astype(bf16), tokens).astype(bf16)
    outgoing_o[...] = chosen.reshape(FAR, HELD, WIDTH)


def select(index, near):
    return pl.pallas_call(
        select_kernel,
        name="select",
        out_shape=[
            jax.ShapeDtypeStruct((FAR, HELD, WIDTH), bf16),
            jax.ShapeDtypeStruct((NEAR * SEQ, ROWS), bf16),
        ],
        in_specs=[pl.BlockSpec(memory_space=pltpu.SMEM), vmem],
        out_specs=[vmem] * 2,
        compiler_params=pltpu.CompilerParams(vmem_limit_bytes=8 * MIB),
    )(index, near)


def swiglu(inputs, w_gate, w_up, w_down):
    hidden = (silu(dot(inputs, w_gate)) * dot(inputs, w_up)).astype(bf16)
    return dot(hidden, w_down)


def expert_kernel(arrived, gate, up, down, back):
    rows = arrived[...].reshape(ROWS, WIDTH)
    out = swiglu(rows, gate[0], up[0], down[0]).astype(bf16)
    back[...] = out.reshape(FAR, HELD, WIDTH)


def experts(arrived, gate, up, down):
    return pl.pallas_call(
        expert_kernel,
        name="experts",
        out_shape=jax.ShapeDtypeStruct(arrived.shape, bf16),
        in_specs=[vmem] * 4,
        out_specs=vmem,
        cost_estimate=pl.CostEstimate(flops=500_000_000, bytes_accessed=3_000_000, transcendentals=0),
        compiler_params=pltpu.CompilerParams(vmem_limit_bytes=8 * MIB),
    )(arrived, gate, up, down)


def offsets(masks):
    found = [0]
    for m in masks:
        found = found + [f ^ m for f in found]
    return found


far_shards = (0, 4)


def dense_kernel(*refs):
    near, other, mix = refs[0:3]
    shards, own_o, other_o = list(refs[3:11]), refs[11], refs[12]
    held, sems = refs[13], refs[14]
    copies = []
    for i, k in enumerate(far_shards):
        copies.append(pltpu.make_async_copy(shards[k], held.at[i], sems.at[i]))
        copies[i].start()
        shards[k] = held.at[i]
    count = NEAR * SEQ
    inputs = jnp.concatenate(
        [t[:, :, 0:WIDTH].reshape(count, WIDTH) for t in (near, other)], axis=0
    )
    for c in copies:
        c.wait()
    n = shards[0].shape[0] // 3
    gates, ups, downs = [
        jnp.concatenate([w[i * n : (i + 1) * n] for w in shards], axis=0) for i in range(3)
    ]
    hidden = (silu(dot_t(inputs, gates)) * dot_t(inputs, ups)).astype(bf16)
    part = (dot(hidden, downs) / (1.0 + jnp.exp(-mix[...]))).astype(bf16)
    own_o[...] = part[0:count].reshape(NEAR, SEQ, WIDTH)
    other_o[...] = part[count:].reshape(NEAR, SEQ, WIDTH)


def dense(near, other, weights, mix):
    weights = [
        pltpu.with_memory_space_constraint(w, pltpu.HBM) if k in far_shards else w
        for k, w in enumerate(weights)
    ]
    part = jax.ShapeDtypeStruct((NEAR, SEQ, WIDTH), bf16)
    return pl.pallas_call(
        dense_kernel,
        name="dense",
        out_shape=[part] * 2,
        in_specs=[vmem] * 3 + [hbm if k in far_shards else vmem for k in range(8)],
        out_specs=[vmem] * 2,
        scratch_shapes=[
            pltpu.VMEM((len(far_shards),) + weights[0].shape, bf16),
            pltpu.SemaphoreType.DMA((len(far_shards),)),
        ],
        cost_estimate=pl.CostEstimate(flops=500_000_000, bytes_accessed=4_000_000, transcendentals=0),
        compiler_params=pltpu.CompilerParams(vmem_limit_bytes=12 * MIB),
    )(near, other, mix[None], *weights)


def combine_kernel(place, back, combine, own, other, keep_o, send_o, total_s):
    rows = back[...].reshape(ROWS, WIDTH)
    total = dot(combine[...], rows).reshape(NEAR, SEQ, WIDTH)
    total_s[...] = total + own[...].astype(f32) + other[...].astype(f32)
    for j, k in enumerate((0, 6, 2, 4)):
        span = slice(j * SEQ, (j + 1) * SEQ)
        keep_o[span] = total_s[place[0] ^ k]
        send_o[span] = total_s[place[0] ^ (k + 1)].astype(bf16)


def halves(rows):
    return [
        jax.ShapeDtypeStruct((rows // 2, WIDTH), f32),
        jax.ShapeDtypeStruct((rows // 2, WIDTH), bf16),
    ]


def combine_near(place, back, combine, own, other):
    return pl.pallas_call(
        combine_kernel,
        name="combine",
        out_shape=halves(NEAR * SEQ),
        in_specs=[pl.BlockSpec(memory_space=pltpu.SMEM)] + [vmem] * 4,
        out_specs=[vmem] * 2,
        scratch_shapes=[pltpu.VMEM((NEAR, SEQ, WIDTH), f32)],
        compiler_params=pltpu.CompilerParams(vmem_limit_bytes=8 * MIB),
    )(place, back, combine, own, other)


def fold_kernel(kept, came, keep_o, send_o):
    total = kept[...] + came[...].astype(f32)
    half = total.shape[0] // 2
    keep_o[...] = total[0:half]
    send_o[...] = total[half:].astype(bf16)


def fold(kept, came):
    return pl.pallas_call(
        fold_kernel,
        name="fold",
        out_shape=halves(kept.shape[0]),
        in_specs=[vmem] * 2,
        out_specs=[vmem] * 2,
        compiler_params=pltpu.CompilerParams(vmem_limit_bytes=2 * MIB),
    )(kept, came)


def shared_kernel(own, s_gate, s_up, s_down, out):
    out[...] = swiglu(own[...], s_gate[...], s_up[...], s_down[...])


def shared(own, s_gate, s_up, s_down):
    return pl.pallas_call(
        shared_kernel,
        name="shared",
        out_shape=jax.ShapeDtypeStruct((SEQ, WIDTH), f32),
        in_specs=[vmem] * 4,
        out_specs=vmem,
        cost_estimate=pl.CostEstimate(flops=900_000_000, bytes_accessed=2_000_000, transcendentals=0),
        compiler_params=pltpu.CompilerParams(vmem_limit_bytes=4 * MIB),
    )(own, s_gate, s_up, s_down)


def final_kernel(kept, came, residual, extra, out):
    combined = extra[...] + kept[...] + came[...].astype(f32)
    out[...] = (residual[...] + normed(combined)).astype(bf16)


def final(kept, came, residual, extra):
    return pl.pallas_call(
        final_kernel,
        name="final",
        out_shape=jax.ShapeDtypeStruct(residual.shape, bf16),
        in_specs=[vmem] * 4,
        out_specs=vmem,
        compiler_params=pltpu.CompilerParams(vmem_limit_bytes=4 * MIB),
    )(kept, came, residual, extra)


near_groups = [[r ^ f for r in offsets(near_masks)] for f in offsets(far_masks)]
far_groups = [[r ^ f for f in offsets(far_masks)] for r in offsets(near_masks)]


def exchange(values, groups):
    return lax.all_to_all(
        values, "ep", split_axis=0, concat_axis=0, axis_index_groups=groups, tiled=True
    )


def per_device(
    tokens,
    lengths,
    cache_keys,
    cache_values,
    retention_state,
    mix_gain,
    query_weight,
    key_weight,
    value_weight,
    out_weight,
    ffn_gain,
    routes,
    route_scores,
    expert_gate,
    expert_up,
    expert_down,
    shared_gate,
    shared_up,
    shared_down,
    dense_gate,
    dense_up,
    dense_down,
    dense_mix,
):
    residual, normal_ffn, new_keys, new_values, outgoing, shard = mixer(
        tokens,
        lengths,
        mix_gain,
        ffn_gain,
        routes,
        route_scores,
        cache_keys,
        cache_values,
        retention_state,
        query_weight,
        key_weight,
        value_weight,
        out_weight,
        dense_gate,
        dense_up,
        dense_down,
    )
    hop = {}
    for m in weight_masks:
        hop[m] = flip(shard, m)
    first, second, third = weight_masks
    for m, k in ((first, second), (second, third), (third, first)):
        hop[m ^ k] = flip(hop[m], k)
    hop[first ^ second ^ third] = flip(hop[first ^ second], third)
    weights = [shard] + list(hop.values())

    near = exchange(outgoing, near_groups)
    place = lax.axis_index("ep").astype(jnp.int32)
    index = place & 7
    chosen, combine = select(index[None], near)
    other = flip(near, wide_mask)
    own_part, other_part = dense(near, other, weights, dense_mix)
    arrived = exchange(chosen, far_groups)
    outputs = experts(arrived, expert_gate, expert_up, expert_down)
    back = exchange(outputs, far_groups)
    other_part = flip(other_part, wide_mask)
    kept, sent = combine_near(index[None], back, combine, own_part, other_part)
    for m in (1, 2):
        came = flip(sent, m)
        kept, sent = fold(kept, came)
    came = flip(sent, 6)
    extra = shared(normal_ffn, shared_gate, shared_up, shared_down)
    layer_out = final(kept, came, residual, extra)
    return (layer_out, new_keys, new_values)


def solution(mesh):
    in_specs = (
        P("ep", None),
        P("ep"),
        P("ep", None, None),
        P("ep", None, None),
        P("ep", None, None, None),
        P(),
        P(),
        P(),
        P(),
        P(),
        P(),
        P("ep", None),
        P("ep", None),
        P("ep", None, None),
        P("ep", None, None),
        P("ep", None, None),
        P(),
        P(),
        P(),
        P("ep", None),
        P("ep", None),
        P("ep", None),
        P(),
    )
    out_specs = (P("ep", None), P("ep", None), P("ep", None))

    return jax.shard_map(
        per_device, mesh=mesh, in_specs=in_specs, out_specs=out_specs, check_vma=False
    )
```
